512 devices in a mesh: dp: 4 (over x), kv: 64 (over z, y), tp: 2 (over core).
Axes of the slice: x: 4, y: 8, z: 8, core: 2. Of those that a mesh axis runs over, the one named last changes fastest.
Arguments:
- tokens: bfloat16 [256, 4096], P('dp', ('kv', 'tp')), parts along dimension 0, may hold values from -16 to 16
- mix_gain: float32 [4096], replicated, may hold values from 0.1 to 1.9
- w_query: bfloat16 [4096, 2048], P('kv', 'tp'), may hold values from -0.09375 to 0.09375
- w_key: bfloat16 [4096, 2048], P('kv', 'tp'), may hold values from -0.09375 to 0.09375
- w_value: bfloat16 [4096, 4096], P('kv', 'tp'), may hold values from -0.09375 to 0.09375
- w_igate: bfloat16 [4096, 16], replicated, may hold values from -0.09375 to 0.09375
- w_fgate: bfloat16 [4096, 16], replicated, may hold values from -0.09375 to 0.09375
- igate_bias: float32 [16], replicated, may hold values from -3 to 1
- fgate_bias: float32 [16], replicated, may hold values from -2 to 5
- memory: float32 [256, 16, 256, 128], P(('dp', 'kv'), 'tp'), parts along dimension 0, may hold values from -6 to 6
- normalizer: float32 [256, 16, 128], P(('dp', 'kv'), 'tp'), parts along dimension 0, may hold values from -6 to 6
- stabilizer: float32 [256, 16], P(('dp', 'kv'), 'tp'), parts along dimension 0, may hold values from -3 to 3
- w_output: bfloat16 [4096, 4096], P('tp', 'kv'), may hold values from -0.09375 to 0.09375
- mlp_gain: float32 [4096], replicated, may hold values from 0.1 to 1.9
- w_up: bfloat16 [4096, 16384], P(None, ('kv', 'tp')), may hold values from -0.09375 to 0.09375
- w_down: bfloat16 [16384, 4096], P(('kv', 'tp')), may hold values from -0.1875 to 0.1875
Outputs:
- new_tokens: bfloat16 [256, 4096], P('dp', ('kv', 'tp')), parts along dimension 0
- new_memory: float32 [256, 16, 256, 128], P(('dp', 'kv'), 'tp'), parts along dimension 0
- new_normalizer: float32 [256, 16, 128], P(('dp', 'kv'), 'tp'), parts along dimension 0
- new_stabilizer: float32 [256, 16], P(('dp', 'kv'), 'tp'), parts along dimension 0
The draws below stay inside these ranges and needn't reach their ends.
There are 4 independent parts, one for each index of `dp`. The reference program is written for one: setup_inputs(seed, part) draws one part's arguments, and reference() takes and returns one part's arrays. A program takes and returns all parts, laid end to end along the dimension named above; an argument that names none is the same for every part. Nothing has to cross between parts.
All inputs are finite; a program needn't handle non-finite values.
Results may differ from the reference program's by a relative error of at most 0.019.
Values may be sent and summed in bfloat16 or wider, within the bound.
No kernel may reach another device: no remote copies, remote signals or barrier semaphores. Data moves between devices by JAX's collectives and lax.ppermute only.
A program may use at most 64 MiB of HBM per device.

```python
import jax
import jax.numpy as jnp
from jax import lax

D = 4096
NH = 16
DV = 256
DQK = 128
FF = 16384
BATCH = 64
N_TP = 2


def with_spikes(array, key, source, target, shards_of, factor):
    def block_of(axis_at):
        return (jnp.arange(array.shape[axis_at]) // (array.shape[axis_at] // shards_of)).reshape((-1,) + (1,) * (array.ndim - 1 - axis_at))

    near = jax.random.permutation(key, shards_of)[block_of(target)]
    far = (block_of(target) + shards_of // 2) % shards_of
    return jnp.where((block_of(source) == near) | (block_of(source) == far), factor * array, array)


def levels(stream_key, shape, split, least, high):
    level, own = 1.0, jax.random.fold_in(stream_key, 6)
    for position, parts in split:
        heights = jnp.exp(jax.random.uniform(jax.random.fold_in(own, position), (parts,), jnp.float32, least / len(split), high / len(split)))
        level = level * jnp.repeat(heights, shape[position] // parts).reshape([-1 if axis == position else 1 for axis in range(len(shape))])
    return level


def bell_draw(stream_key, dims, width, most, cuts=(), dtype=jnp.bfloat16):
    values = jax.random.normal(stream_key, dims, jnp.float32) * width
    if len(cuts) > 0:
        values = levels(stream_key, dims, cuts, -0.22, 0.18) * values
    return jnp.clip(values, min=-most, max=most).astype(dtype)


def gaussian_with(key, shape, spread, reach, cuts, heavy, dtype=jnp.bfloat16):
    drawn = spread * jax.random.normal(key, shape, jnp.float32)
    if cuts:
        drawn = drawn * levels(key, shape, cuts, -0.22, 0.18)
    return jnp.clip(with_spikes(drawn, jax.random.fold_in(key, 3), *heavy), -reach, reach).astype(dtype)


def setup_inputs(seed: int = 0, part: int = 0) -> dict:
    key_of = jax.random.split(jax.random.key(seed), 17)
    part_splits = jax.random.split(jax.random.fold_in(key_of[16], part), 17)
    tokens = gaussian_with(part_splits[0], (BATCH, D), 1.0, 16.0, ((1, 128),), (1, 0, 64, 4.0))
    mix_gain = jnp.clip(1.0 + 0.18 * jax.random.normal(key_of[1], (D,), jnp.float32), 0.1, 1.9)
    w_query = bell_draw(key_of[2], (D, NH * DQK), D ** -0.5, 0.09375, ((0, 64), (1, 2)))
    w_key = bell_draw(key_of[3], (D, NH * DQK), D ** -0.5, 0.09375, ((0, 64), (1, 2)))
    w_value = bell_draw(key_of[4], (D, NH * DV), D ** -0.5, 0.09375, ((0, 64), (1, 2)))
    w_igate = bell_draw(key_of[5], (D, NH), D ** -0.5, 0.09375)
    w_fgate = bell_draw(key_of[6], (D, NH), D ** -0.5, 0.09375)
    igate_bias = jnp.clip(jax.random.uniform(key_of[7], (NH,), jnp.float32, -3.0, 1.0), -3.0, 1.0)
    fgate_bias = jnp.clip(jax.random.uniform(key_of[8], (NH,), jnp.float32, -2.0, 5.0), -2.0, 5.0)
    memory = bell_draw(part_splits[9], (BATCH, NH, DV, DQK), 1.0, 6.0, ((0, 64), (1, 2)), jnp.float32)
    normalizer = bell_draw(part_splits[10], (BATCH, NH, DQK), 1.0, 6.0, ((0, 64), (1, 2)), jnp.float32)
    stabilizer = jnp.clip(jax.random.uniform(part_splits[11], (BATCH, NH), jnp.float32, -3.0, 3.0) * levels(part_splits[11], (BATCH, NH), ((0, 64), (1, 2)), -0.4, 0.0), -3.0, 3.0)
    w_output = bell_draw(key_of[12], (NH * DV, D), (NH * DV) ** -0.5, 0.09375, ((0, 2), (1, 64)))
    mlp_gain = jnp.clip(1.0 + 0.18 * jax.random.normal(key_of[13], (D,), jnp.float32), 0.1, 1.9)
    w_up = bell_draw(key_of[14], (D, FF), D ** -0.5, 0.09375, ((1, 128),))
    w_down = gaussian_with(key_of[15], (FF, D), FF ** -0.5, 0.1875, ((0, 128),), (0, 1, 128, 5.5))
    return {"tokens": tokens, "mix_gain": mix_gain, "w_query": w_query, "w_key": w_key, "w_value": w_value, "w_igate": w_igate, "w_fgate": w_fgate, "igate_bias": igate_bias, "fgate_bias": fgate_bias, "memory": memory, "normalizer": normalizer, "stabilizer": stabilizer, "w_output": w_output, "mlp_gain": mlp_gain, "w_up": w_up, "w_down": w_down}


norm_eps = 1e-06

def rms_normed(rows, gain):
    wide_rows = rows.astype(jnp.float32)
    scale = lax.rsqrt(lax.optimization_barrier(jnp.mean(wide_rows * wide_rows, axis=-1, keepdims=True)) + norm_eps)
    return (wide_rows * scale * gain).astype(jnp.bfloat16)

def reference(tokens, mix_gain, w_query, w_key, w_value, w_igate, w_fgate, igate_bias, fgate_bias, memory, normalizer, stabilizer, w_output, mlp_gain, w_up, w_down):
    batch_rows = tokens.shape[0]
    normed = rms_normed(tokens, mix_gain)
    queries = (jnp.dot(normed, w_query, preferred_element_type=jnp.float32) * DQK ** (-0.5)).reshape(batch_rows, NH, DQK)
    key_rows = jnp.dot(normed, w_key, preferred_element_type=jnp.float32).reshape(batch_rows, NH, DQK)
    values = jnp.dot(normed, w_value, preferred_element_type=jnp.float32).reshape(batch_rows, NH, DV)
    input_gate = jnp.dot(normed, w_igate, preferred_element_type=jnp.float32) + igate_bias
    log_forget = jax.nn.log_sigmoid(jnp.dot(normed, w_fgate, preferred_element_type=jnp.float32) + fgate_bias)
    carried = log_forget + stabilizer
    new_stabilizer = jnp.maximum(carried, input_gate)
    keep_weight = jnp.exp(carried - new_stabilizer)
    fresh_weight = jnp.exp(input_gate - new_stabilizer)
    recall = jnp.einsum('bhvd,bhd->bhv', memory, queries, precision=lax.Precision.HIGHEST)
    match_score = lax.optimization_barrier(jnp.sum(queries * key_rows, axis=-1))
    numerator = keep_weight[..., None] * recall + (fresh_weight * match_score)[..., None] * values
    denominator = keep_weight * lax.optimization_barrier(jnp.sum(normalizer * queries, axis=-1)) + fresh_weight * match_score
    floor_value = jnp.maximum(jnp.abs(denominator), jnp.exp(-new_stabilizer))
    cell_out = (numerator / floor_value[..., None]).astype(jnp.bfloat16).reshape(batch_rows, NH * DV)
    new_memory = keep_weight[..., None, None] * memory + fresh_weight[..., None, None] * values[..., :, None] * key_rows[..., None, :]
    new_normalizer = keep_weight[..., None] * normalizer + fresh_weight[..., None] * key_rows
    half_width = NH * DV // N_TP
    summed = tokens.astype(jnp.float32)
    for half_index in range(N_TP):
        half_out = jnp.dot(cell_out[:, half_index * half_width:(half_index + 1) * half_width], w_output[half_index * half_width:(half_index + 1) * half_width], preferred_element_type=jnp.float32).astype(jnp.bfloat16)
        half_out = lax.optimization_barrier(half_out)
        summed = summed + half_out.astype(jnp.float32)
    middle = summed.astype(jnp.bfloat16)
    mixer_in = rms_normed(middle, mlp_gain)
    up_rows = jnp.dot(mixer_in, w_up, preferred_element_type=jnp.float32)
    activation = jnp.square(jax.nn.relu(up_rows)).astype(jnp.bfloat16)
    down_rows = jnp.dot(activation, w_down, preferred_element_type=jnp.float32)
    new_tokens = (middle.astype(jnp.float32) + down_rows).astype(jnp.bfloat16)
    return (new_tokens, new_memory, new_normalizer, new_stabilizer)
```

```python
import jax
import jax.numpy as jnp
from jax import lax
from jax.experimental import pallas as pl
from jax.experimental.pallas import tpu as pltpu
from jax.sharding import PartitionSpec as P

DV = 256
DQK = 128
LANES = 128
NORM_EPS = 1e-06
PITCH = 40

F32 = jnp.float32
BF16 = jnp.bfloat16

NT = (((1,), (1,)), ((), ()))

TN = (((0,), (0,)), ((), ()))


def split(wide):
    high = wide.astype(BF16)
    return high, (wide - high.astype(F32)).astype(BF16)


vmem = pl.BlockSpec(memory_space=pltpu.VMEM)
smem = pl.BlockSpec(memory_space=pltpu.SMEM)


def project_kernel(kv_pos, packed, gain, wq, wk, wv, wig, wfg, out, rows):
    n = packed.shape[1] // 2
    block = kv_pos[0] // 2
    odd = kv_pos[0] % 2
    wide = packed[...].astype(F32)
    x = jnp.concatenate([wide[:, :n].T, wide[:, n:].T], axis=1)
    twice = jnp.concatenate([x, x], axis=1)
    lane = lax.broadcasted_iota(jnp.int32, twice.shape, 1)
    mine = (lane // n) == odd
    scaled = jnp.where(mine, twice * gain[pl.ds(block, 1), :], 0.0)
    wide_lhs = scaled.astype(BF16)
    folded = scaled[:, :n] + scaled[:, n:]
    lhs = folded.astype(BF16)
    start = pl.multiple_of(block * LANES, LANES)
    ig = wig[:, pl.ds(start, LANES)]
    fg = wfg[:, pl.ds(start, LANES)]
    gates = jnp.concatenate([ig, fg, ig, fg, jnp.zeros((LANES - 4 * ig.shape[0], LANES), BF16)], axis=0)
    sums = lax.dot_general(wide_lhs, gates, NT, preferred_element_type=F32)
    squares = jnp.sum(x * x, axis=1, keepdims=True)
    sums = jnp.where(lane >= n, jnp.broadcast_to(squares, sums.shape), sums)
    low = ((lane >= n // 2) & (lane < n)) | (lane == n + 1)
    sums = jnp.where(low, sums - sums.astype(BF16).astype(F32), sums)
    for at in range(32, 40):
        rows[pl.ds(at, n, stride=PITCH), :] = sums

    def place(w, first, step):
        cols = w.shape[1]
        for c in range(0, cols, 256):
            part = jnp.dot(lhs, w[:, c : c + 256], preferred_element_type=F32)
            for half in range(2):
                tile = c // LANES + half
                at = first + (tile if step == 1 else (tile % 2) * 8 + tile // 2)
                rows[pl.ds(at, n, stride=PITCH), :] = part[:, half * LANES : (half + 1) * LANES]

    place(wq, 0, 1)
    place(wk, 8, 1)
    place(wv, 16, 2)
    for r in range(n):
        out[r] = rows[r * PITCH : r * PITCH + PITCH, :].astype(BF16)


def cell_kernel(tp_pos, arrived, memory, normalizer, stab, ibias, fbias, out, memory_out, norm_out, stab_out):
    tp = tp_pos[0]
    count = arrived.shape[0]

    def add(i, acc):
        for j in range(8):
            acc = acc + arrived[i * 8 + j].astype(F32)
        return acc

    acc = lax.fori_loop(0, count // 8, add, jnp.zeros((PITCH, LANES), F32))
    lane = lax.broadcasted_iota(jnp.int32, (8, LANES), 1)
    sub = lax.broadcasted_iota(jnp.int32, (8, LANES), 0)
    extra = jnp.broadcast_to(acc[32:33], (8, LANES))
    squares = jnp.sum(jnp.where((lane == 64) | (lane == 65), extra, 0.0), axis=1, keepdims=True)
    scale = lax.rsqrt(squares * (1.0 / 4096.0) + NORM_EPS)
    pad8 = jnp.zeros((1, LANES - 8), F32)
    pad16 = jnp.zeros((1, LANES - 32), F32)
    bias = jnp.concatenate([ibias[...], fbias[...], pad16], axis=1)
    gates = extra * scale + bias
    head = tp * 8 + sub
    igate = jnp.sum(jnp.where((lane == head) | (lane == head + 32), gates, 0.0), axis=1, keepdims=True)
    fgate = jnp.sum(jnp.where((lane == head + 16) | (lane == head + 48), gates, 0.0), axis=1, keepdims=True)
    old = jnp.sum(jnp.where(lane == sub, jnp.concatenate([stab[...], pad8], axis=1), 0.0), axis=1, keepdims=True)
    log_forget = jnp.minimum(fgate, 0.0) - jnp.log1p(jnp.exp(-jnp.abs(fgate)))
    carried = log_forget + old
    new = jnp.maximum(carried, igate)
    keep = jnp.exp(carried - new)
    fresh = jnp.exp(igate - new)
    stab_out[...] = jnp.sum(jnp.where(lane == sub, new, 0.0), axis=0, keepdims=True)[:, :8]
    q = acc[0:8] * (scale * DQK ** (-0.5))
    k = acc[8:16] * scale
    v = jnp.concatenate([acc[16:24], acc[24:32]], axis=1) * scale
    q_both = jnp.concatenate(split(q), axis=0)
    sub2 = lax.broadcasted_iota(jnp.int32, (8, DV), 0)
    recall = jnp.zeros((8, DV), F32)
    for h in range(8):
        part = lax.dot_general(q_both, memory[h].astype(BF16), NT, preferred_element_type=F32)
        recall = jnp.where(sub2 == h, part[:8] + part[8:], recall)
    match = jnp.sum(q * k, axis=1, keepdims=True)
    old_norm = normalizer[...]
    denominator = keep * jnp.sum(old_norm * q, axis=1, keepdims=True) + fresh * match
    floor = jnp.maximum(jnp.abs(denominator), jnp.exp(-new))
    cell = (keep * recall + (fresh * match) * v) / floor
    tile = jnp.concatenate([cell[:, :LANES], cell[:, LANES:]], axis=0).astype(BF16)
    for r in range(count):
        out[r] = tile
    norm_out[...] = keep * old_norm + fresh * k
    value = fresh * v
    v_high, v_low = split(value)
    k_high, k_low = split(k)
    for h in range(8):
        row = slice(h, h + 1)
        left = jnp.concatenate([v_high[row], v_high[row], v_low[row]], axis=0)
        right = jnp.concatenate([k_high[row], k_low[row], k_high[row]], axis=0)
        outer = lax.dot_general(left, right, TN, preferred_element_type=F32)
        memory_out[h] = keep[row] * memory[h] + outer


def output_kernel(arrived, w, out, rows):
    count = arrived.shape[0]
    for r in range(count):
        rows[r * 16 : r * 16 + 16, :] = arrived[r].astype(F32)
    parts = []
    for tile in range(16):
        c = (tile % 2) * 8 + tile // 2
        parts.append(rows[pl.ds(c, count, stride=16), :].astype(BF16))
    acc = lax.dot_general(w[...], jnp.concatenate(parts, axis=1), NT, preferred_element_type=F32)
    half = acc.shape[0] // 2
    out[...] = jnp.concatenate([acc[:half], acc[half:]], axis=1)


def mixer_kernel(middle, w_up, w_down, out):
    n = middle.shape[1] // 2
    x = middle[...]
    wide = x.astype(F32)
    squares = jnp.sum(wide * wide, axis=0, keepdims=True)
    squares = squares[:, :n] + squares[:, n:]
    scale = lax.rsqrt(squares * (1.0 / 4096.0) + NORM_EPS)
    both = jnp.dot(w_up[...], x, preferred_element_type=F32)
    hidden = both.shape[0] // 2
    up = (both[:hidden, :n] + both[hidden:, n:]) * scale
    act = jnp.square(jnp.maximum(up, 0.0))
    zero = jnp.zeros_like(act)
    rhs = jnp.concatenate(
        [jnp.concatenate([act, zero], axis=1), jnp.concatenate([zero, act], axis=1)], axis=0
    ).astype(BF16)
    for i in range(0, w_down.shape[0], 256):
        out[i : i + 256, :] = jnp.dot(w_down[i : i + 256, :], rhs, preferred_element_type=F32).astype(BF16)


def call(kernel, shapes, *args, scalars=0, scratch=()):
    outs = [jax.ShapeDtypeStruct(s, d) for s, d in shapes]
    many = len(outs) > 1
    return pl.pallas_call(
        kernel,
        out_shape=outs if many else outs[0],
        in_specs=[smem] * scalars + [vmem] * (len(args) - scalars),
        out_specs=[vmem] * len(outs) if many else vmem,
        scratch_shapes=list(scratch),
        compiler_params=pltpu.CompilerParams(vmem_limit_bytes=16 * 1024 * 1024),
    )(*args)


def on_device(
    tokens,
    mix_gain,
    w_query,
    w_key,
    w_value,
    w_igate,
    w_fgate,
    igate_bias,
    fgate_bias,
    memory,
    normalizer,
    stabilizer,
    w_output,
    mlp_gain,
    w_up,
    w_down,
):
    kv = lax.axis_size("kv")
    kv_index = lax.axis_index("kv")
    tp_index = lax.axis_index("tp")
    rows, thin = tokens.shape
    kv_pos = kv_index.astype(jnp.int32).reshape(1)
    tp_pos = tp_index.astype(jnp.int32).reshape(1)
    thin_t = tokens.T
    side = lax.broadcasted_iota(jnp.int32, (thin, 2 * rows), 1) // rows
    padded = jnp.where(side == tp_index, jnp.concatenate([thin_t, thin_t], axis=1), jnp.zeros((), BF16))
    packed = lax.psum(padded, "tp")

    hidden = w_up.shape[1]
    up_t = (w_up.astype(F32) * mlp_gain[:, None]).astype(BF16)
    up_t = up_t.reshape(kv, 2, thin, hidden).transpose(1, 3, 0, 2).reshape(2 * hidden, kv * thin)
    down_t = w_down.reshape(hidden, kv, 2, thin).transpose(1, 3, 2, 0).reshape(kv * thin, 2 * hidden)

    sends = call(
        project_kernel,
        [((rows, PITCH, LANES), BF16)],
        kv_pos,
        packed,
        mix_gain.reshape(-1, LANES),
        w_query,
        w_key,
        w_value,
        w_igate.T,
        w_fgate.T,
        scalars=1,
        scratch=[pltpu.VMEM((rows * PITCH, LANES), F32)],
    )
    arrived = lax.all_to_all(sends, "kv", 0, 0, tiled=True)
    arrived, up_t, down_t = lax.optimization_barrier((arrived, up_t, down_t))
    cell, new_memory, new_normalizer, new_stabilizer = call(
        cell_kernel,
        [
            ((kv, 16, LANES), BF16),
            ((8, DV, DQK), F32),
            ((8, DQK), F32),
            ((1, 8), F32),
        ],
        tp_pos,
        arrived,
        memory[0],
        normalizer[0],
        stabilizer,
        igate_bias[None],
        fgate_bias[None],
        scalars=1,
    )
    cells = lax.all_to_all(cell, "kv", 0, 0, tiled=True)

    half = call(
        output_kernel,
        [((thin, 2 * rows), F32)],
        cells,
        w_output.T,
        scratch=[pltpu.VMEM((rows * 16, LANES), F32)],
    )
    middle = (packed.astype(F32) + lax.psum(half, "tp")).astype(BF16)
    middles = lax.all_to_all(
        jnp.broadcast_to(middle[None], (kv, thin, 2 * rows)), "kv", 0, 0, tiled=True
    )
    downs = call(
        mixer_kernel,
        [((kv * thin, 2 * rows), BF16)],
        middles.reshape(kv * thin, 2 * rows),
        up_t,
        down_t,
    )
    back = lax.all_to_all(downs.reshape(kv, thin, 2 * rows), "kv", 0, 0, tiled=True)
    total = lax.psum(jnp.sum(back.astype(F32), axis=0), "tp") + middle.astype(F32)
    own = jnp.where(tp_index == 0, total[:, :rows], total[:, rows:])
    new_tokens = own.astype(BF16).T
    return (new_tokens, new_memory[None], new_normalizer[None], new_stabilizer)


def solution(mesh):
    in_specs = (
        P("dp", ("kv", "tp")),
        P(),
        P("kv", "tp"),
        P("kv", "tp"),
        P("kv", "tp"),
        P(),
        P(),
        P(),
        P(),
        P(("dp", "kv"), "tp", None, None),
        P(("dp", "kv"), "tp", None),
        P(("dp", "kv"), "tp"),
        P("tp", "kv"),
        P(),
        P(None, ("kv", "tp")),
        P(("kv", "tp"), None),
    )
    out_specs = (
        P("dp", ("kv", "tp")),
        P(("dp", "kv"), "tp", None, None),
        P(("dp", "kv"), "tp", None),
        P(("dp", "kv"), "tp"),
    )
    return jax.shard_map(
        on_device, mesh=mesh, in_specs=in_specs, out_specs=out_specs, check_vma=False
    )
```

```python
import jax
import jax.numpy as jnp
from jax import lax
from jax.experimental import pallas as pl
from jax.experimental.pallas import tpu as pltpu
from jax.sharding import PartitionSpec as P

DV = 256
DQK = 128
LANES = 128
NORM_EPS = 1e-06
PITCH = 40

F32 = jnp.float32
BF16 = jnp.bfloat16

NT = (((1,), (1,)), ((), ()))

TN = (((0,), (0,)), ((), ()))


def split(wide):
    high = wide.astype(BF16)
    return high, (wide - high.astype(F32)).astype(BF16)


vmem = pl.BlockSpec(memory_space=pltpu.VMEM)
smem = pl.BlockSpec(memory_space=pltpu.SMEM)


any_space = pl.BlockSpec(memory_space=pl.ANY)


def fetch_kernel(kv_pos, tp_pos, tokens, gain, wq, wk, wv, wig, wfg, padded, *rest):
    outs, sems = rest[:-1], rest[-1]
    own, outs = outs[-1], outs[:-1]
    start = pl.multiple_of(kv_pos[0] // 2 * LANES, LANES)
    sources = (tokens, gain, wq, wk, wv, wig.at[:, pl.ds(start, LANES)], wfg.at[:, pl.ds(start, LANES)])
    copies = [pltpu.make_async_copy(src, dst, sems.at[i]) for i, (src, dst) in enumerate(zip(sources, (own, *outs)))]
    for copy in copies:
        copy.start()
    copies[0].wait()
    x = own[...].astype(F32)
    twice = jnp.concatenate([x, x], axis=1)
    padded[...] = jnp.where(halves_of(twice) == tp_pos[0], twice, 0.0).astype(BF16)
    for copy in copies[1:]:
        copy.wait()


def project_kernel(kv_pos, packed, gain, wq, wk, wv, wig, wfg, out, rows):
    n = packed.shape[1] // 2
    block = kv_pos[0] // 2
    odd = kv_pos[0] % 2
    wide = packed[...].astype(F32)
    x = jnp.concatenate([wide[:, :n].T, wide[:, n:].T], axis=1)
    twice = jnp.concatenate([x, x], axis=1)
    lane = lax.broadcasted_iota(jnp.int32, twice.shape, 1)
    mine = (lane // n) == odd
    scaled = jnp.where(mine, twice * gain[pl.ds(block, 1), :], 0.0)
    wide_lhs = scaled.astype(BF16)
    folded = scaled[:, :n] + scaled[:, n:]
    lhs = folded.astype(BF16)
    ig = wig[...]
    fg = wfg[...]
    gates = jnp.concatenate([ig, fg, ig, fg, jnp.zeros((LANES - 4 * ig.shape[0], LANES), BF16)], axis=0)
    sums = lax.dot_general(wide_lhs, gates, NT, preferred_element_type=F32)
    squares = jnp.sum(x * x, axis=1, keepdims=True)
    sums = jnp.where(lane >= n, jnp.broadcast_to(squares, sums.shape), sums)
    low = ((lane >= n // 2) & (lane < n)) | (lane == n + 1)
    sums = jnp.where(low, sums - sums.astype(BF16).astype(F32), sums)
    for at in range(32, 40):
        rows[pl.ds(at, n, stride=PITCH), :] = sums

    def place(w, first, step):
        cols = w.shape[1]
        for c in range(0, cols, 256):
            part = jnp.dot(lhs, w[:, c : c + 256], preferred_element_type=F32)
            for half in range(2):
                tile = c // LANES + half
                at = first + (tile if step == 1 else (tile % 2) * 8 + tile // 2)
                rows[pl.ds(at, n, stride=PITCH), :] = part[:, half * LANES : (half + 1) * LANES]

    place(wq, 0, 1)
    place(wk, 8, 1)
    place(wv, 16, 2)
    for r in range(n):
        out[r] = rows[r * PITCH : r * PITCH + PITCH, :].astype(BF16)


def cell_kernel(tp_pos, arrived, normalizer, small, memory_in, out, norm_out, stab_out, memory_out, memory, sems):
    tp = tp_pos[0]
    heads = memory.shape[0]
    loads = [pltpu.make_async_copy(memory_in.at[h], memory.at[h], sems.at[h]) for h in range(heads)]
    stores = [pltpu.make_async_copy(memory.at[h], memory_out.at[h], sems.at[heads + h]) for h in range(heads)]
    for load in loads:
        load.start()
    count = arrived.shape[0]

    def add(i, acc):
        for j in range(8):
            acc = acc + arrived[i * 8 + j].astype(F32)
        return acc

    acc = lax.fori_loop(0, count // 8, add, jnp.zeros((PITCH, LANES), F32))
    lane = lax.broadcasted_iota(jnp.int32, (8, LANES), 1)
    sub = lax.broadcasted_iota(jnp.int32, (8, LANES), 0)
    extra = jnp.broadcast_to(acc[32:33], (8, LANES))
    squares = jnp.sum(jnp.where((lane == 64) | (lane == 65), extra, 0.0), axis=1, keepdims=True)
    scale = lax.rsqrt(squares * (1.0 / 4096.0) + NORM_EPS)
    gates = extra * scale + small[0:1, :]
    head = tp * 8 + sub
    igate = jnp.sum(jnp.where((lane == head) | (lane == head + 32), gates, 0.0), axis=1, keepdims=True)
    fgate = jnp.sum(jnp.where((lane == head + 16) | (lane == head + 48), gates, 0.0), axis=1, keepdims=True)
    old = jnp.sum(jnp.where(lane == sub, small[1:2, :], 0.0), axis=1, keepdims=True)
    log_forget = jnp.minimum(fgate, 0.0) - jnp.log1p(jnp.exp(-jnp.abs(fgate)))
    carried = log_forget + old
    new = jnp.maximum(carried, igate)
    keep = jnp.exp(carried - new)
    fresh = jnp.exp(igate - new)
    stab_out[...] = jnp.sum(jnp.where(lane == sub, new, 0.0), axis=0, keepdims=True)[:, :8]
    q = acc[0:8] * (scale * DQK ** (-0.5))
    k = acc[8:16] * scale
    v = jnp.concatenate([acc[16:24], acc[24:32]], axis=1) * scale
    q_both = jnp.concatenate(split(q), axis=0)
    sub2 = lax.broadcasted_iota(jnp.int32, (8, DV), 0)
    recall = jnp.zeros((8, DV), F32)
    for h in range(heads):
        loads[h].wait()
        part = lax.dot_general(q_both, memory[h].astype(BF16), NT, preferred_element_type=F32)
        recall = jnp.where(sub2 == h, part[:8] + part[8:], recall)
    match = jnp.sum(q * k, axis=1, keepdims=True)
    old_norm = normalizer[...]
    denominator = keep * jnp.sum(old_norm * q, axis=1, keepdims=True) + fresh * match
    floor = jnp.maximum(jnp.abs(denominator), jnp.exp(-new))
    cell = (keep * recall + (fresh * match) * v) / floor
    tile = jnp.concatenate([cell[:, :LANES], cell[:, LANES:]], axis=0).astype(BF16)
    for r in range(count):
        out[r] = tile
    norm_out[...] = keep * old_norm + fresh * k
    value = fresh * v
    v_high, v_low = split(value)
    k_high, k_low = split(k)
    for h in range(heads):
        row = slice(h, h + 1)
        left = jnp.concatenate([v_high[row], v_high[row], v_low[row]], axis=0)
        right = jnp.concatenate([k_high[row], k_low[row], k_high[row]], axis=0)
        outer = lax.dot_general(left, right, TN, preferred_element_type=F32)
        memory[h] = keep[row] * memory[h] + outer
        stores[h].start()
    for store in stores:
        store.wait()


def output_kernel(arrived, w, out, rows):
    count = arrived.shape[0]
    for r in range(count):
        rows[r * 16 : r * 16 + 16, :] = arrived[r].astype(F32)
    parts = []
    for tile in range(16):
        c = (tile % 2) * 8 + tile // 2
        parts.append(rows[pl.ds(c, count, stride=16), :].astype(BF16))
    acc = lax.dot_general(w[...], jnp.concatenate(parts, axis=1), NT, preferred_element_type=F32)
    half = acc.shape[0] // 2
    out[...] = jnp.concatenate([acc[:half], acc[half:]], axis=1)


def prepare_kernel(tp_pos, w_up, gain, w_down, stab, ibias, fbias, normalizer, w_out, keep, send, small, *rest):
    outs, turned, sems = rest[:-2], rest[-2], rest[-1]
    copies = [
        pltpu.make_async_copy(src, dst, sems.at[i])
        for i, (src, dst) in enumerate(zip((normalizer, w_out), outs))
    ]
    for copy in copies:
        copy.start()
    small[...] = jnp.zeros(small.shape, F32)
    small[0:1, 0:16] = ibias[...]
    small[0:1, 16:32] = fbias[...]
    small[1:2, 0:8] = stab[...]
    tp = tp_pos[0]
    chips = w_up.shape[0]
    for k in range(0, chips, 2):
        turned[k : k + 2] = w_down[:, k * 64 : k * 64 + 128].T.reshape(2, 2, 2, 16, 128)
    for side in range(2):
        dst = (keep, send)[side]
        half = (tp + side) % 2
        for quarter in range(2):
            lanes = slice(quarter * 128, quarter * 128 + 128)
            factors = gain[pl.ds(half * 2 + quarter, 1), :]
            for block in range(4):
                part = w_up[block * 16 : block * 16 + 16, half, quarter].reshape(256, 128).T
                part = part.astype(F32) * factors[:, block * 256 : block * 256 + 256]
                dst[block * 256 + quarter * 128 : block * 256 + quarter * 128 + 128, :] = part.astype(BF16)
            dst[1024:2048, lanes] = turned[:, half, quarter].reshape(1024, 128)
    for copy in copies:
        copy.wait()


def middle_kernel(tp_pos, half_sum, packed, out, own):
    tp = tp_pos[0]
    whole = packed[...].astype(F32) + half_sum[...]
    n = whole.shape[1] // 2
    mine = jnp.where(tp == 0, whole[:, :n], whole[:, n:])
    thin = mine.shape[0] // 2
    tile = jnp.concatenate([mine[:thin], mine[thin:]], axis=1).astype(BF16)
    own[...] = tile
    for r in range(out.shape[0]):
        out[r] = tile


def halves_of(like):
    return (lax.broadcasted_iota(jnp.int32, like.shape, 1) >= like.shape[1] // 2).astype(jnp.int32)


def swapped(wide):
    n = wide.shape[1] // 2
    return jnp.concatenate([wide[:, n:], wide[:, :n]], axis=1)


def up_kernel(tp_pos, middle, keep, other, out):
    tp = tp_pos[0]
    wide = middle[...].astype(F32)
    squares = jnp.sum(wide * wide, axis=0, keepdims=True)

    def product(w):
        acc = jnp.zeros((256, 128), F32)
        for block in range(4):
            rows = slice(block * 256, block * 256 + 256)
            acc = acc + jnp.dot(w[rows, :], middle[rows, :], preferred_element_type=F32)
        low = acc[:128] + swapped(acc[128:])
        return jnp.where(halves_of(low) == 0, low, swapped(low))

    own = product(keep)
    out[:128] = jnp.where(halves_of(own) == tp, own, product(other))
    out[128:] = jnp.broadcast_to(squares + swapped(squares), (8, 128))


def down_kernel(tp_pos, near, far_sums, keep, other, out):
    tp = tp_pos[0]
    sums = near[...] + far_sums[...]
    scale = lax.rsqrt(sums[128:129] * (1.0 / 4096.0) + NORM_EPS)
    act = jnp.square(jnp.maximum(sums[:128] * scale, 0.0))
    swap = swapped(act)
    side = halves_of(act)

    def spread(rows):
        return jnp.concatenate([jnp.where(side == 0, rows, 0.0), jnp.where(side == 1, rows, 0.0)], axis=0).astype(BF16)

    own = spread(jnp.where(side == tp, act, swap))
    far = spread(jnp.where(side == tp, swap, act))
    for i in range(0, 1024, 256):
        rows = slice(1024 + i, 1280 + i)
        part = jnp.dot(keep[rows, :], own, preferred_element_type=F32)
        part = part + jnp.dot(other[rows, :], far, preferred_element_type=F32)
        out[i : i + 256, :] = part.astype(BF16)


def finish_kernel(back, own, out):
    def add(i, acc):
        for j in range(8):
            acc = acc + back[i * 8 + j].astype(F32)
        return acc

    acc = lax.fori_loop(0, back.shape[0] // 8, add, own[...].astype(F32))
    n = acc.shape[1] // 2
    out[...] = jnp.concatenate([acc[:, :n], acc[:, n:]], axis=0).astype(BF16)


def call(kernel, shapes, *args, scalars=0, far=0, fetched=0, away=(), scratch=()):
    outs = [jax.ShapeDtypeStruct(s, d) if i in away else pltpu.VMEM(s, d) for i, (s, d) in enumerate(shapes)]
    out_specs = [vmem] * (len(outs) - fetched) + [any_space] * fetched
    many = len(outs) > 1
    near = len(args) - far
    args = args[:near] + tuple(pltpu.with_memory_space_constraint(x, pltpu.HBM) for x in args[near:])
    return pl.pallas_call(
        kernel,
        out_shape=outs if many else outs[0],
        in_specs=[smem] * scalars + [vmem] * (near - scalars) + [any_space] * far,
        out_specs=out_specs if many else out_specs[0],
        scratch_shapes=list(scratch),
        compiler_params=pltpu.CompilerParams(vmem_limit_bytes=16 * 1024 * 1024),
    )(*args)


def on_device(
    tokens,
    mix_gain,
    w_query,
    w_key,
    w_value,
    w_igate,
    w_fgate,
    igate_bias,
    fgate_bias,
    memory,
    normalizer,
    stabilizer,
    w_output,
    mlp_gain,
    w_up,
    w_down,
):
    kv = lax.axis_size("kv")
    kv_index = lax.axis_index("kv")
    tp_index = lax.axis_index("tp")
    rows, thin = tokens.shape
    kv_pos = kv_index.astype(jnp.int32).reshape(1)
    tp_pos = tp_index.astype(jnp.int32).reshape(1)
    padded, gain_near, wq, wk, wv, ig, fg = call(
        fetch_kernel,
        [
            ((thin, 2 * rows), BF16),
            ((mix_gain.shape[0] // LANES, LANES), F32),
            (w_query.shape, BF16),
            (w_key.shape, BF16),
            (w_value.shape, BF16),
            ((w_igate.shape[1], LANES), BF16),
            ((w_fgate.shape[1], LANES), BF16),
        ],
        kv_pos,
        tp_pos,
        tokens.T,
        mix_gain.reshape(-1, LANES),
        w_query,
        w_key,
        w_value,
        w_igate.T,
        w_fgate.T,
        scalars=2,
        far=7,
        fetched=6,
        scratch=[pltpu.VMEM((thin, rows), BF16), pltpu.SemaphoreType.DMA((7,))],
    )
    packed = lax.psum(padded, "tp")

    hidden = w_up.shape[1]
    quarter = thin // 2
    gains = mlp_gain.reshape(kv, 2, 2, quarter).transpose(1, 2, 0, 3).reshape(4, kv * quarter)
    keep, send, small, state_norm, w_out = call(
        prepare_kernel,
        [
            ((2048, 256), BF16),
            ((2048, 256), BF16),
            ((8, LANES), F32),
            (normalizer.shape[1:], F32),
            (w_output.shape[::-1], BF16),
        ],
        tp_pos,
        w_up.reshape(kv, 2, 2, quarter, hidden),
        gains,
        w_down,
        stabilizer,
        igate_bias[None],
        fgate_bias[None],
        normalizer[0],
        w_output.T,
        scalars=1,
        far=2,
        fetched=2,
        scratch=[pltpu.VMEM((kv, 2, 2, quarter, hidden), BF16), pltpu.SemaphoreType.DMA((2,))],
    )
    other = lax.ppermute(send, "tp", [(0, 1), (1, 0)])

    sends = call(
        project_kernel,
        [((rows, PITCH, LANES), BF16)],
        kv_pos,
        packed,
        gain_near,
        wq,
        wk,
        wv,
        ig,
        fg,
        scalars=1,
        away=(0,),
        scratch=[pltpu.VMEM((rows * PITCH, LANES), F32)],
    )
    arrived = lax.all_to_all(sends, "kv", 0, 0, tiled=True)
    arrived, keep, other = lax.optimization_barrier((arrived, keep, other))
    cell, new_normalizer, new_stabilizer, new_memory = call(
        cell_kernel,
        [
            ((kv, 16, LANES), BF16),
            ((8, DQK), F32),
            ((1, 8), F32),
            (memory.shape[1:], F32),
        ],
        tp_pos,
        arrived,
        state_norm,
        small,
        memory[0],
        scalars=1,
        far=1,
        fetched=1,
        away=(1, 2, 3),
        scratch=[pltpu.VMEM(memory.shape[1:], F32), pltpu.SemaphoreType.DMA((16,))],
    )
    cells = lax.all_to_all(cell, "kv", 0, 0, tiled=True)

    half = call(
        output_kernel,
        [((thin, 2 * rows), F32)],
        cells,
        w_out,
        scratch=[pltpu.VMEM((rows * 16, LANES), F32)],
    )
    middle, own = call(
        middle_kernel,
        [((kv, quarter, 2 * rows), BF16), ((quarter, 2 * rows), BF16)],
        tp_pos,
        lax.psum(half, "tp"),
        packed,
        scalars=1,
    )
    middles = lax.all_to_all(middle, "kv", 0, 0, tiled=True).reshape(kv * quarter, 2 * rows)
    sums = call(up_kernel, [((136, 128), F32)], tp_pos, middles, keep, other, scalars=1)
    downs = call(
        down_kernel,
        [((kv * quarter, 2 * rows), BF16)],
        tp_pos,
        sums,
        lax.ppermute(sums, "tp", [(0, 1), (1, 0)]),
        keep,
        other,
        scalars=1,
    )
    back = lax.all_to_all(downs.reshape(kv, quarter, 2 * rows), "kv", 0, 0, tiled=True)
    new_tokens = call(finish_kernel, [((thin, rows), BF16)], back, own, away=(0,)).T
    return (new_tokens, new_memory[None], new_normalizer[None], new_stabilizer)


def solution(mesh):
    in_specs = (
        P("dp", ("kv", "tp")),
        P(),
        P("kv", "tp"),
        P("kv", "tp"),
        P("kv", "tp"),
        P(),
        P(),
        P(),
        P(),
        P(("dp", "kv"), "tp", None, None),
        P(("dp", "kv"), "tp", None),
        P(("dp", "kv"), "tp"),
        P("tp", "kv"),
        P(),
        P(None, ("kv", "tp")),
        P(("kv", "tp"), None),
    )
    out_specs = (
        P("dp", ("kv", "tp")),
        P(("dp", "kv"), "tp", None, None),
        P(("dp", "kv"), "tp", None),
        P(("dp", "kv"), "tp"),
    )
    return jax.shard_map(
        on_device, mesh=mesh, in_specs=in_specs, out_specs=out_specs, check_vma=False
    )
```

```python
import jax
import jax.numpy as jnp
from jax import lax
from jax.experimental import pallas as pl
from jax.experimental.pallas import tpu as pltpu
from jax.sharding import PartitionSpec as P


DV = 256
DQK = 128
LANES = 128
NORM_EPS = 1e-06
PITCH = 40

F32 = jnp.float32
BF16 = jnp.bfloat16

NT = (((1,), (1,)), ((), ()))

TN = (((0,), (0,)), ((), ()))


def split(wide):
    high = wide.astype(BF16)
    return high, (wide - high.astype(F32)).astype(BF16)


vmem = pl.BlockSpec(memory_space=pltpu.VMEM)
smem = pl.BlockSpec(memory_space=pltpu.SMEM)


any_space = pl.BlockSpec(memory_space=pl.ANY)


def fetch_kernel(kv_pos, tp_pos, tokens, gain, wq, wk, wv, wig, wfg, padded, *rest):
    outs, sems = rest[:-1], rest[-1]
    start = pl.multiple_of(kv_pos[0] // 2 * LANES, LANES)
    sources = (tokens, gain, wq, wk, wv, wig.at[:, pl.ds(start, LANES)], wfg.at[:, pl.ds(start, LANES)])
    copies = [pltpu.make_async_copy(src, dst, sems.at[i]) for i, (src, dst) in enumerate(zip(sources, outs))]
    for copy in copies:
        copy.start()
    copies[0].wait()
    x = outs[0][...].astype(F32)
    twice = jnp.concatenate([x, x], axis=1)
    padded[...] = jnp.where(halves_of(twice) == tp_pos[0], twice, 0.0).astype(BF16)
    for copy in copies[1:]:
        copy.wait()


def project_kernel(kv_pos, packed, gain, wq, wk, wv, wig, wfg, *rest):
    sources, out, held, rows, sems = rest[:5], rest[5], rest[6:11], rest[11], rest[12]
    copies = [pltpu.make_async_copy(src, dst, sems.at[i]) for i, (src, dst) in enumerate(zip(sources, held))]
    for copy in copies:
        copy.start()
    n = packed.shape[1] // 2
    block = kv_pos[0] // 2
    odd = kv_pos[0] % 2
    wide = packed[...].astype(F32)
    x = jnp.concatenate([wide[:, :n].T, wide[:, n:].T], axis=1)
    twice = jnp.concatenate([x, x], axis=1)
    lane = lax.broadcasted_iota(jnp.int32, twice.shape, 1)
    mine = (lane // n) == odd
    scaled = jnp.where(mine, twice * gain[pl.ds(block, 1), :], 0.0)
    wide_lhs = scaled.astype(BF16)
    folded = scaled[:, :n] + scaled[:, n:]
    lhs = folded.astype(BF16)
    ig = wig[...]
    fg = wfg[...]
    gates = jnp.concatenate([ig, fg, ig, fg, jnp.zeros((LANES - 4 * ig.shape[0], LANES), BF16)], axis=0)
    sums = lax.dot_general(wide_lhs, gates, NT, preferred_element_type=F32)
    squares = jnp.sum(x * x, axis=1, keepdims=True)
    sums = jnp.where(lane >= n, jnp.broadcast_to(squares, sums.shape), sums)
    low = ((lane >= n // 2) & (lane < n)) | (lane == n + 1)
    sums = jnp.where(low, sums - sums.astype(BF16).astype(F32), sums)
    for at in range(32, 40):
        rows[pl.ds(at, n, stride=PITCH), :] = sums

    def place(w, first, step):
        cols = w.shape[1]
        for c in range(0, cols, 256):
            part = jnp.dot(lhs, w[:, c : c + 256], preferred_element_type=F32)
            for half in range(2):
                tile = c // LANES + half
                at = first + (tile if step == 1 else (tile % 2) * 8 + tile // 2)
                rows[pl.ds(at, n, stride=PITCH), :] = part[:, half * LANES : (half + 1) * LANES]

    place(wq, 0, 1)
    place(wk, 8, 1)
    place(wv, 16, 2)
    for r in range(n):
        out[r] = rows[r * PITCH : r * PITCH + PITCH, :].astype(BF16)
    for copy in copies:
        copy.wait()


def cell_kernel(tp_pos, arrived, memory, normalizer, stab, ibias, fbias, gain, *rest):
    out, keys, vals, keeps, norm_out, stab_out, gain_out, sem = rest
    copy = pltpu.make_async_copy(gain, gain_out, sem)
    copy.start()
    tp = tp_pos[0]
    heads = memory.shape[0]
    pad = jnp.zeros((1, LANES - 32), F32)
    bias = jnp.concatenate([ibias[...], fbias[...], pad], axis=1)
    old_stab = jnp.concatenate([stab[...], jnp.zeros((1, LANES - 8), F32)], axis=1)
    count = arrived.shape[0]

    def add(i, acc):
        for j in range(8):
            acc = acc + arrived[i * 8 + j].astype(F32)
        return acc

    acc = lax.fori_loop(0, count // 8, add, jnp.zeros((PITCH, LANES), F32))
    lane = lax.broadcasted_iota(jnp.int32, (8, LANES), 1)
    sub = lax.broadcasted_iota(jnp.int32, (8, LANES), 0)
    extra = jnp.broadcast_to(acc[32:33], (8, LANES))
    squares = jnp.sum(jnp.where((lane == 64) | (lane == 65), extra, 0.0), axis=1, keepdims=True)
    scale = lax.rsqrt(squares * (1.0 / 4096.0) + NORM_EPS)
    gates = extra * scale + bias
    head = tp * 8 + sub
    igate = jnp.sum(jnp.where((lane == head) | (lane == head + 32), gates, 0.0), axis=1, keepdims=True)
    fgate = jnp.sum(jnp.where((lane == head + 16) | (lane == head + 48), gates, 0.0), axis=1, keepdims=True)
    old = jnp.sum(jnp.where(lane == sub, old_stab, 0.0), axis=1, keepdims=True)
    log_forget = jnp.minimum(fgate, 0.0) - jnp.log1p(jnp.exp(-jnp.abs(fgate)))
    carried = log_forget + old
    new = jnp.maximum(carried, igate)
    keep = jnp.exp(carried - new)
    fresh = jnp.exp(igate - new)
    stab_out[...] = jnp.sum(jnp.where(lane == sub, new, 0.0), axis=0, keepdims=True)[:, :8]
    q = acc[0:8] * (scale * DQK ** (-0.5))
    k = acc[8:16] * scale
    v = jnp.concatenate([acc[16:24], acc[24:32]], axis=1) * scale
    q_both = jnp.concatenate(split(q), axis=0)
    sub2 = lax.broadcasted_iota(jnp.int32, (8, DV), 0)
    recall = jnp.zeros((8, DV), F32)
    for h in range(heads):
        part = lax.dot_general(q_both, memory[h].astype(BF16), NT, preferred_element_type=F32)
        recall = jnp.where(sub2 == h, part[:8] + part[8:], recall)
    match = jnp.sum(q * k, axis=1, keepdims=True)
    old_norm = normalizer[...]
    denominator = keep * jnp.sum(old_norm * q, axis=1, keepdims=True) + fresh * match
    floor = jnp.maximum(jnp.abs(denominator), jnp.exp(-new))
    cell = (keep * recall + (fresh * match) * v) / floor
    tile = jnp.concatenate([cell[:, :LANES], cell[:, LANES:]], axis=0).astype(BF16)
    for r in range(count):
        out[r] = tile
    norm_out[...] = keep * old_norm + fresh * k
    keys[...] = k
    vals[...] = fresh * v
    keeps[...] = jnp.broadcast_to(keep, keeps.shape)
    copy.wait()


def update_kernel(keys, vals, keeps, memory_in, memory_out, memory, sems):
    heads = memory.shape[0]
    loads = [pltpu.make_async_copy(memory_in.at[h], memory.at[h], sems.at[h]) for h in range(heads)]
    stores = [pltpu.make_async_copy(memory.at[h], memory_out.at[h], sems.at[heads + h]) for h in range(heads)]
    for load in loads:
        load.start()
    v_high, v_low = split(vals[...])
    k_high, k_low = split(keys[...])
    for h in range(heads):
        row = slice(h, h + 1)
        left = jnp.concatenate([v_high[row], v_high[row], v_low[row]], axis=0)
        right = jnp.concatenate([k_high[row], k_low[row], k_high[row]], axis=0)
        outer = lax.dot_general(left, right, TN, preferred_element_type=F32)
        loads[h].wait()
        memory[h] = keeps[row, :] * memory[h] + outer
        stores[h].start()
    for store in stores:
        store.wait()


def folded(wide):
    thin = wide.shape[0] // 2
    return jnp.concatenate([wide[:thin], wide[thin:]], axis=1)


def output_kernel(tp_pos, arrived, w, own, out, rows):
    tp = tp_pos[0]
    count = arrived.shape[0]
    for r in range(count):
        rows[r * 16 : r * 16 + 16, :] = arrived[r].astype(F32)
    parts = []
    for tile in range(16):
        c = (tile % 2) * 8 + tile // 2
        parts.append(rows[pl.ds(c, count, stride=16), :].astype(BF16))
    acc = lax.dot_general(w[...], jnp.concatenate(parts, axis=1), NT, preferred_element_type=F32)
    half = acc.shape[0] // 2
    first = folded(acc[:half])
    second = folded(acc[half:])
    own[...] = jnp.where(tp == 0, first, second).astype(BF16)
    out[...] = jnp.concatenate([jnp.where(tp == 1, first, 0.0), jnp.where(tp == 0, second, 0.0)], axis=0).astype(BF16)


def prepare_kernel(tp_pos, w_up, gain, w_down, w_out, keep, send, held, turned, sem):
    copy = pltpu.make_async_copy(w_out, held, sem)
    copy.start()
    tp = tp_pos[0]
    chips = w_up.shape[0]
    for k in range(0, chips, 2):
        turned[k : k + 2] = w_down[:, k * 64 : k * 64 + 128].T.reshape(2, 2, 2, 16, 128)
    for side in range(2):
        dst = (keep, send)[side]
        half = (tp + side) % 2
        for quarter in range(2):
            lanes = slice(quarter * 128, quarter * 128 + 128)
            factors = gain[pl.ds(half * 2 + quarter, 1), :]
            for block in range(4):
                part = w_up[block * 16 : block * 16 + 16, half, quarter].reshape(256, 128).T
                part = part.astype(F32) * factors[:, block * 256 : block * 256 + 256]
                dst[block * 256 + quarter * 128 : block * 256 + quarter * 128 + 128, :] = part.astype(BF16)
            dst[1024:2048, lanes] = turned[:, half, quarter].reshape(1024, 128)
    copy.wait()


def middle_kernel(tp_pos, half, both, tokens, out, own):
    tp = tp_pos[0]
    thin = half.shape[0]
    other = jnp.where(tp == 0, both[:thin].astype(F32), both[thin:].astype(F32))
    tile = (folded(tokens[...].astype(F32)) + half[...].astype(F32) + other).astype(BF16)
    own[...] = tile
    for r in range(out.shape[0]):
        out[r] = tile


def halves_of(like):
    return (lax.broadcasted_iota(jnp.int32, like.shape, 1) >= like.shape[1] // 2).astype(jnp.int32)


def swapped(wide):
    n = wide.shape[1] // 2
    return jnp.concatenate([wide[:, n:], wide[:, :n]], axis=1)


def up_kernel(tp_pos, middle, keep, other, out):
    tp = tp_pos[0]
    wide = middle[...].astype(F32)
    squares = jnp.sum(wide * wide, axis=0, keepdims=True)

    def product(w):
        acc = jnp.zeros((256, 128), F32)
        for block in range(4):
            rows = slice(block * 256, block * 256 + 256)
            acc = acc + jnp.dot(w[rows, :], middle[rows, :], preferred_element_type=F32)
        low = acc[:128] + swapped(acc[128:])
        return jnp.where(halves_of(low) == 0, low, swapped(low))

    own = product(keep)
    out[:128] = jnp.where(halves_of(own) == tp, own, product(other))
    out[128:] = jnp.broadcast_to(squares + swapped(squares), (8, 128))


def down_kernel(tp_pos, near, far_sums, keep, other, out):
    tp = tp_pos[0]
    sums = near[...] + far_sums[...]
    scale = lax.rsqrt(sums[128:129] * (1.0 / 4096.0) + NORM_EPS)
    act = jnp.square(jnp.maximum(sums[:128] * scale, 0.0))
    swap = swapped(act)
    side = halves_of(act)

    def spread(rows):
        return jnp.concatenate([jnp.where(side == 0, rows, 0.0), jnp.where(side == 1, rows, 0.0)], axis=0).astype(BF16)

    own = spread(jnp.where(side == tp, act, swap))
    far = spread(jnp.where(side == tp, swap, act))
    for i in range(0, 1024, 256):
        rows = slice(1024 + i, 1280 + i)
        part = jnp.dot(keep[rows, :], own, preferred_element_type=F32)
        part = part + jnp.dot(other[rows, :], far, preferred_element_type=F32)
        out[i : i + 256, :] = part.astype(BF16)


def finish_kernel(back, own, out):
    def add(i, acc):
        for j in range(8):
            acc = acc + back[i * 8 + j].astype(F32)
        return acc

    acc = lax.fori_loop(0, back.shape[0] // 8, add, own[...].astype(F32))
    n = acc.shape[1] // 2
    out[...] = jnp.concatenate([acc[:, :n], acc[:, n:]], axis=0).astype(BF16)


def call(kernel, shapes, *args, scalars=0, far=0, fetched=0, away=(), scratch=()):
    outs = [pltpu.HBM(s, d) if i in away else pltpu.VMEM(s, d) for i, (s, d) in enumerate(shapes)]
    out_specs = [vmem] * (len(outs) - fetched) + [any_space] * fetched
    many = len(outs) > 1
    near = len(args) - far
    args = args[:near] + tuple(pltpu.with_memory_space_constraint(x, pltpu.HBM) for x in args[near:])
    return pl.pallas_call(
        kernel,
        out_shape=outs if many else outs[0],
        in_specs=[smem] * scalars + [vmem] * (near - scalars) + [any_space] * far,
        out_specs=out_specs if many else out_specs[0],
        scratch_shapes=list(scratch),
        compiler_params=pltpu.CompilerParams(vmem_limit_bytes=16 * 1024 * 1024),
    )(*args)


def on_device(
    tokens,
    mix_gain,
    w_query,
    w_key,
    w_value,
    w_igate,
    w_fgate,
    igate_bias,
    fgate_bias,
    memory,
    normalizer,
    stabilizer,
    w_output,
    mlp_gain,
    w_up,
    w_down,
):
    kv = lax.axis_size("kv")
    kv_index = lax.axis_index("kv")
    tp_index = lax.axis_index("tp")
    rows, thin = tokens.shape
    kv_pos = kv_index.astype(jnp.int32).reshape(1)
    tp_pos = tp_index.astype(jnp.int32).reshape(1)
    padded, own_tokens, gain_near, wq, wk, wv, ig, fg = call(
        fetch_kernel,
        [
            ((thin, 2 * rows), BF16),
            ((thin, rows), BF16),
            ((mix_gain.shape[0] // LANES, LANES), F32),
            (w_query.shape, BF16),
            (w_key.shape, BF16),
            (w_value.shape, BF16),
            ((w_igate.shape[1], LANES), BF16),
            ((w_fgate.shape[1], LANES), BF16),
        ],
        kv_pos,
        tp_pos,
        tokens.T,
        mix_gain.reshape(-1, LANES),
        w_query,
        w_key,
        w_value,
        w_igate.T,
        w_fgate.T,
        scalars=2,
        far=7,
        fetched=6,
        scratch=[pltpu.SemaphoreType.DMA((7,))],
    )
    packed = lax.psum(padded, "tp")

    sends, state, state_norm, old_stab, ibias, fbias = call(
        project_kernel,
        [
            ((rows, PITCH, LANES), BF16),
            (memory.shape[1:], F32),
            (normalizer.shape[1:], F32),
            (stabilizer.shape, F32),
            ((1, igate_bias.shape[0]), F32),
            ((1, fgate_bias.shape[0]), F32),
        ],
        kv_pos,
        packed,
        gain_near,
        wq,
        wk,
        wv,
        ig,
        fg,
        memory[0],
        normalizer[0],
        stabilizer,
        igate_bias[None],
        fgate_bias[None],
        scalars=1,
        far=5,
        fetched=5,
        scratch=[pltpu.VMEM((rows * PITCH, LANES), F32), pltpu.SemaphoreType.DMA((5,))],
    )
    arrived = lax.all_to_all(sends, "kv", 0, 0, tiled=True)
    cell, keys, vals, keeps, new_normalizer, new_stabilizer, late_gain = call(
        cell_kernel,
        [
            ((kv, 16, LANES), BF16),
            ((8, DQK), F32),
            ((8, DV), F32),
            ((8, LANES), F32),
            ((8, DQK), F32),
            ((1, 8), F32),
            ((mlp_gain.shape[0] // LANES, LANES), F32),
        ],
        tp_pos,
        arrived,
        state,
        state_norm,
        old_stab,
        ibias,
        fbias,
        mlp_gain.reshape(-1, LANES),
        scalars=1,
        far=1,
        fetched=1,
        away=(0, 4, 5),
        scratch=[pltpu.SemaphoreType.DMA],
    )
    cells = lax.all_to_all(cell, "kv", 0, 0, tiled=True)
    new_memory = call(
        update_kernel,
        [(memory.shape[1:], F32)],
        keys,
        vals,
        keeps,
        memory[0],
        far=1,
        fetched=1,
        away=(0,),
        scratch=[pltpu.VMEM(memory.shape[1:], F32), pltpu.SemaphoreType.DMA((16,))],
    )

    hidden = w_up.shape[1]
    quarter = thin // 2
    gains = late_gain.reshape(kv, 2, 2, quarter).transpose(1, 2, 0, 3).reshape(4, kv * quarter)
    keep, send, w_out = call(
        prepare_kernel,
        [((2048, 256), BF16), ((2048, 256), BF16), (w_output.shape[::-1], BF16)],
        tp_pos,
        w_up.reshape(kv, 2, 2, quarter, hidden),
        gains,
        w_down,
        w_output.T,
        scalars=1,
        far=1,
        fetched=1,
        away=(1,),
        scratch=[pltpu.VMEM((kv, 2, 2, quarter, hidden), BF16), pltpu.SemaphoreType.DMA],
    )
    other = lax.ppermute(send, "tp", [(0, 1), (1, 0)])
    cells, keep, other, new_memory = lax.optimization_barrier((cells, keep, other, new_memory))

    half, crossing = call(
        output_kernel,
        [((quarter, 2 * rows), BF16), ((thin, 2 * rows), BF16)],
        tp_pos,
        cells,
        w_out,
        scalars=1,
        scratch=[pltpu.VMEM((rows * 16, LANES), F32)],
    )
    middle, own = call(
        middle_kernel,
        [((kv, quarter, 2 * rows), BF16), ((quarter, 2 * rows), BF16)],
        tp_pos,
        half,
        lax.psum(crossing, "tp"),
        own_tokens,
        scalars=1,
    )
    middles = lax.all_to_all(middle, "kv", 0, 0, tiled=True).reshape(kv * quarter, 2 * rows)
    sums = call(up_kernel, [((136, 128), F32)], tp_pos, middles, keep, other, scalars=1)
    downs = call(
        down_kernel,
        [((kv * quarter, 2 * rows), BF16)],
        tp_pos,
        sums,
        lax.ppermute(sums, "tp", [(0, 1), (1, 0)]),
        keep,
        other,
        scalars=1,
    )
    back = lax.all_to_all(downs.reshape(kv, quarter, 2 * rows), "kv", 0, 0, tiled=True)
    new_tokens = call(finish_kernel, [((thin, rows), BF16)], back, own, away=(0,)).T
    return (new_tokens, new_memory[None], new_normalizer[None], new_stabilizer)


def solution(mesh):
    in_specs = (
        P("dp", ("kv", "tp")),
        P(),
        P("kv", "tp"),
        P("kv", "tp"),
        P("kv", "tp"),
        P(),
        P(),
        P(),
        P(),
        P(("dp", "kv"), "tp", None, None),
        P(("dp", "kv"), "tp", None),
        P(("dp", "kv"), "tp"),
        P("tp", "kv"),
        P(),
        P(None, ("kv", "tp")),
        P(("kv", "tp"), None),
    )
    out_specs = (
        P("dp", ("kv", "tp")),
        P(("dp", "kv"), "tp", None, None),
        P(("dp", "kv"), "tp", None),
        P(("dp", "kv"), "tp"),
    )
    return jax.shard_map(on_device, mesh=mesh, in_specs=in_specs, out_specs=out_specs, check_vma=False)
```

```python
import jax
import jax.numpy as jnp
from jax import lax
from jax.experimental import pallas as pl
from jax.experimental.pallas import tpu as pltpu
from jax.sharding import PartitionSpec as P


DV = 256
DQK = 128
LANES = 128
NORM_EPS = 1e-06
PITCH = 40

F32 = jnp.float32
BF16 = jnp.bfloat16

NT = (((1,), (1,)), ((), ()))

TN = (((0,), (0,)), ((), ()))


def split(wide):
    high = wide.astype(BF16)
    return high, (wide - high.astype(F32)).astype(BF16)


vmem = pl.BlockSpec(memory_space=pltpu.VMEM)
smem = pl.BlockSpec(memory_space=pltpu.SMEM)


any_space = pl.BlockSpec(memory_space=pl.ANY)


def fetch_kernel(kv_pos, tp_pos, tokens, gain, wq, wk, wv, wig, wfg, padded, *rest):
    outs, sems = rest[:-1], rest[-1]
    start = pl.multiple_of(kv_pos[0] // 2 * LANES, LANES)
    sources = (tokens, gain, wq, wk, wv, wig.at[:, pl.ds(start, LANES)], wfg.at[:, pl.ds(start, LANES)])
    copies = [pltpu.make_async_copy(src, dst, sems.at[i]) for i, (src, dst) in enumerate(zip(sources, outs))]
    for copy in copies:
        copy.start()
    copies[0].wait()
    x = outs[0][...].astype(F32)
    twice = jnp.concatenate([x, x], axis=1)
    padded[...] = jnp.where(halves_of(twice) == tp_pos[0], twice, 0.0).astype(BF16)
    for copy in copies[1:]:
        copy.wait()


def project_kernel(kv_pos, packed, gain, wq, wk, wv, wig, wfg, *rest):
    sources, out, held, rows, sems = rest[:4], rest[4], rest[5:9], rest[9], rest[10]
    copies = [pltpu.make_async_copy(src, dst, sems.at[i]) for i, (src, dst) in enumerate(zip(sources, held))]
    for copy in copies:
        copy.start()
    n = packed.shape[1] // 2
    block = kv_pos[0] // 2
    odd = kv_pos[0] % 2
    wide = packed[...].astype(F32)
    x = jnp.concatenate([wide[:, :n].T, wide[:, n:].T], axis=1)
    twice = jnp.concatenate([x, x], axis=1)
    lane = lax.broadcasted_iota(jnp.int32, twice.shape, 1)
    mine = (lane // n) == odd
    scaled = jnp.where(mine, twice * gain[pl.ds(block, 1), :], 0.0)
    wide_lhs = scaled.astype(BF16)
    folded = scaled[:, :n] + scaled[:, n:]
    lhs = folded.astype(BF16)
    ig = wig[...]
    fg = wfg[...]
    gates = jnp.concatenate([ig, fg, ig, fg, jnp.zeros((LANES - 4 * ig.shape[0], LANES), BF16)], axis=0)
    sums = lax.dot_general(wide_lhs, gates, NT, preferred_element_type=F32)
    squares = jnp.sum(x * x, axis=1, keepdims=True)
    sums = jnp.where(lane >= n, jnp.broadcast_to(squares, sums.shape), sums)
    low = ((lane >= n // 2) & (lane < n)) | (lane == n + 1)
    sums = jnp.where(low, sums - sums.astype(BF16).astype(F32), sums)
    for at in range(32, 40):
        rows[pl.ds(at, n, stride=PITCH), :] = sums

    def place(w, first, step):
        cols = w.shape[1]
        for c in range(0, cols, 256):
            part = jnp.dot(lhs, w[:, c : c + 256], preferred_element_type=F32)
            for half in range(2):
                tile = c // LANES + half
                at = first + (tile if step == 1 else (tile % 2) * 8 + tile // 2)
                rows[pl.ds(at, n, stride=PITCH), :] = part[:, half * LANES : (half + 1) * LANES]

    place(wq, 0, 1)
    place(wk, 8, 1)
    place(wv, 16, 2)
    for r in range(n):
        out[r] = rows[r * PITCH : r * PITCH + PITCH, :].astype(BF16)
    for copy in copies:
        copy.wait()


def cell_kernel(tp_pos, arrived, normalizer, stab, ibias, fbias, memory_in, *rest):
    out, keys, vals, keeps, norm_out, stab_out, memory, sems = rest
    tp = tp_pos[0]
    heads = memory.shape[0]
    loads = [pltpu.make_async_copy(memory_in.at[h], memory.at[h], sems.at[h]) for h in range(heads)]
    for load in loads:
        load.start()
    pad = jnp.zeros((1, LANES - 32), F32)
    bias = jnp.concatenate([ibias[...], fbias[...], pad], axis=1)
    old_stab = jnp.concatenate([stab[...], jnp.zeros((1, LANES - 8), F32)], axis=1)
    count = arrived.shape[0]

    def add(i, acc):
        for j in range(8):
            acc = acc + arrived[i * 8 + j].astype(F32)
        return acc

    acc = lax.fori_loop(0, count // 8, add, jnp.zeros((PITCH, LANES), F32))
    lane = lax.broadcasted_iota(jnp.int32, (8, LANES), 1)
    sub = lax.broadcasted_iota(jnp.int32, (8, LANES), 0)
    extra = jnp.broadcast_to(acc[32:33], (8, LANES))
    squares = jnp.sum(jnp.where((lane == 64) | (lane == 65), extra, 0.0), axis=1, keepdims=True)
    scale = lax.rsqrt(squares * (1.0 / 4096.0) + NORM_EPS)
    gates = extra * scale + bias
    head = tp * 8 + sub
    igate = jnp.sum(jnp.where((lane == head) | (lane == head + 32), gates, 0.0), axis=1, keepdims=True)
    fgate = jnp.sum(jnp.where((lane == head + 16) | (lane == head + 48), gates, 0.0), axis=1, keepdims=True)
    old = jnp.sum(jnp.where(lane == sub, old_stab, 0.0), axis=1, keepdims=True)
    log_forget = jnp.minimum(fgate, 0.0) - jnp.log1p(jnp.exp(-jnp.abs(fgate)))
    carried = log_forget + old
    new = jnp.maximum(carried, igate)
    keep = jnp.exp(carried - new)
    fresh = jnp.exp(igate - new)
    stab_out[...] = jnp.sum(jnp.where(lane == sub, new, 0.0), axis=0, keepdims=True)[:, :8]
    q = acc[0:8] * (scale * DQK ** (-0.5))
    k = acc[8:16] * scale
    v = jnp.concatenate([acc[16:24], acc[24:32]], axis=1) * scale
    q_both = jnp.concatenate(split(q), axis=0)
    sub2 = lax.broadcasted_iota(jnp.int32, (8, DV), 0)
    recall = jnp.zeros((8, DV), F32)
    for h in range(heads):
        loads[h].wait()
        part = lax.dot_general(q_both, memory[h].astype(BF16), NT, preferred_element_type=F32)
        recall = jnp.where(sub2 == h, part[:8] + part[8:], recall)
    match = jnp.sum(q * k, axis=1, keepdims=True)
    old_norm = normalizer[...]
    denominator = keep * jnp.sum(old_norm * q, axis=1, keepdims=True) + fresh * match
    floor = jnp.maximum(jnp.abs(denominator), jnp.exp(-new))
    cell = (keep * recall + (fresh * match) * v) / floor
    tile = jnp.concatenate([cell[:, :LANES], cell[:, LANES:]], axis=0).astype(BF16)
    for r in range(count):
        out[r] = tile
    norm_out[...] = keep * old_norm + fresh * k
    keys[...] = k
    vals[...] = fresh * v
    keeps[...] = jnp.broadcast_to(keep, keeps.shape)


def update_kernel(keys, vals, keeps, memory_in, memory_out, memory, sems):
    heads = memory.shape[0]
    loads = [pltpu.make_async_copy(memory_in.at[h], memory.at[h], sems.at[h]) for h in range(heads)]
    stores = [pltpu.make_async_copy(memory.at[h], memory_out.at[h], sems.at[heads + h]) for h in range(heads)]
    for load in loads:
        load.start()
    v_high, v_low = split(vals[...])
    k_high, k_low = split(keys[...])
    for h in range(heads):
        row = slice(h, h + 1)
        left = jnp.concatenate([v_high[row], v_high[row], v_low[row]], axis=0)
        right = jnp.concatenate([k_high[row], k_low[row], k_high[row]], axis=0)
        outer = lax.dot_general(left, right, TN, preferred_element_type=F32)
        loads[h].wait()
        memory[h] = keeps[row, :] * memory[h] + outer
        stores[h].start()
    for store in stores:
        store.wait()


def folded(wide):
    thin = wide.shape[0] // 2
    return jnp.concatenate([wide[:thin], wide[thin:]], axis=1)


def output_kernel(tp_pos, arrived, w, own, out, rows):
    tp = tp_pos[0]
    count = arrived.shape[0]
    for r in range(count):
        rows[r * 16 : r * 16 + 16, :] = arrived[r].astype(F32)
    parts = []
    for tile in range(16):
        c = (tile % 2) * 8 + tile // 2
        parts.append(rows[pl.ds(c, count, stride=16), :].astype(BF16))
    acc = lax.dot_general(w[...], jnp.concatenate(parts, axis=1), NT, preferred_element_type=F32)
    half = acc.shape[0] // 2
    first = folded(acc[:half])
    second = folded(acc[half:])
    own[...] = jnp.where(tp == 0, first, second).astype(BF16)
    out[...] = jnp.concatenate([jnp.where(tp == 1, first, 0.0), jnp.where(tp == 0, second, 0.0)], axis=0).astype(BF16)


def prepare_kernel(tp_pos, w_up, gain, w_down, w_out, keep, send, held, turned, sem):
    copy = pltpu.make_async_copy(w_out, held, sem)
    copy.start()
    tp = tp_pos[0]
    chips = w_up.shape[0]
    for k in range(0, chips, 2):
        turned[k : k + 2] = w_down[:, k * 64 : k * 64 + 128].T.reshape(2, 2, 2, 16, 128)
    for side in range(2):
        dst = (keep, send)[side]
        half = (tp + side) % 2
        for quarter in range(2):
            lanes = slice(quarter * 128, quarter * 128 + 128)
            factors = gain[pl.ds(half * 2 + quarter, 1), :]
            for block in range(4):
                part = w_up[block * 16 : block * 16 + 16, half, quarter].reshape(256, 128).T
                part = part.astype(F32) * factors[:, block * 256 : block * 256 + 256]
                dst[block * 256 + quarter * 128 : block * 256 + quarter * 128 + 128, :] = part.astype(BF16)
            dst[1024:2048, lanes] = turned[:, half, quarter].reshape(1024, 128)
    copy.wait()


def middle_kernel(tp_pos, half, both, tokens, out, own):
    tp = tp_pos[0]
    thin = half.shape[0]
    other = jnp.where(tp == 0, both[:thin].astype(F32), both[thin:].astype(F32))
    tile = (folded(tokens[...].astype(F32)) + half[...].astype(F32) + other).astype(BF16)
    own[...] = tile
    for r in range(out.shape[0]):
        out[r] = tile


def halves_of(like):
    return (lax.broadcasted_iota(jnp.int32, like.shape, 1) >= like.shape[1] // 2).astype(jnp.int32)


def swapped(wide):
    n = wide.shape[1] // 2
    return jnp.concatenate([wide[:, n:], wide[:, :n]], axis=1)


def up_kernel(tp_pos, middle, keep, other, out):
    tp = tp_pos[0]
    wide = middle[...].astype(F32)
    squares = jnp.sum(wide * wide, axis=0, keepdims=True)

    def product(w):
        acc = jnp.zeros((256, 128), F32)
        for block in range(4):
            rows = slice(block * 256, block * 256 + 256)
            acc = acc + jnp.dot(w[rows, :], middle[rows, :], preferred_element_type=F32)
        low = acc[:128] + swapped(acc[128:])
        return jnp.where(halves_of(low) == 0, low, swapped(low))

    own = product(keep)
    out[:128] = jnp.where(halves_of(own) == tp, own, product(other))
    out[128:] = jnp.broadcast_to(squares + swapped(squares), (8, 128))


def down_kernel(tp_pos, near, far_sums, keep, other, out):
    tp = tp_pos[0]
    sums = near[...] + far_sums[...]
    scale = lax.rsqrt(sums[128:129] * (1.0 / 4096.0) + NORM_EPS)
    act = jnp.square(jnp.maximum(sums[:128] * scale, 0.0))
    swap = swapped(act)
    side = halves_of(act)

    def spread(rows):
        return jnp.concatenate([jnp.where(side == 0, rows, 0.0), jnp.where(side == 1, rows, 0.0)], axis=0).astype(BF16)

    own = spread(jnp.where(side == tp, act, swap))
    far = spread(jnp.where(side == tp, swap, act))
    for i in range(0, 1024, 256):
        rows = slice(1024 + i, 1280 + i)
        part = jnp.dot(keep[rows, :], own, preferred_element_type=F32)
        part = part + jnp.dot(other[rows, :], far, preferred_element_type=F32)
        out[i : i + 256, :] = part.astype(BF16)


def finish_kernel(back, own, out):
    def add(i, acc):
        for j in range(8):
            acc = acc + back[i * 8 + j].astype(F32)
        return acc

    acc = lax.fori_loop(0, back.shape[0] // 8, add, own[...].astype(F32))
    n = acc.shape[1] // 2
    out[...] = jnp.concatenate([acc[:, :n], acc[:, n:]], axis=0).astype(BF16)


def call(kernel, shapes, *args, scalars=0, far=0, fetched=0, away=(), scratch=()):
    outs = [pltpu.HBM(s, d) if i in away else pltpu.VMEM(s, d) for i, (s, d) in enumerate(shapes)]
    out_specs = [vmem] * (len(outs) - fetched) + [any_space] * fetched
    many = len(outs) > 1
    near = len(args) - far
    args = args[:near] + tuple(pltpu.with_memory_space_constraint(x, pltpu.HBM) for x in args[near:])
    return pl.pallas_call(
        kernel,
        out_shape=outs if many else outs[0],
        in_specs=[smem] * scalars + [vmem] * (near - scalars) + [any_space] * far,
        out_specs=out_specs if many else out_specs[0],
        scratch_shapes=list(scratch),
        compiler_params=pltpu.CompilerParams(vmem_limit_bytes=16 * 1024 * 1024),
    )(*args)


def on_device(
    tokens,
    mix_gain,
    w_query,
    w_key,
    w_value,
    w_igate,
    w_fgate,
    igate_bias,
    fgate_bias,
    memory,
    normalizer,
    stabilizer,
    w_output,
    mlp_gain,
    w_up,
    w_down,
):
    kv = lax.axis_size("kv")
    kv_index = lax.axis_index("kv")
    tp_index = lax.axis_index("tp")
    rows, thin = tokens.shape
    kv_pos = kv_index.astype(jnp.int32).reshape(1)
    tp_pos = tp_index.astype(jnp.int32).reshape(1)
    padded, own_tokens, gain_near, wq, wk, wv, ig, fg = call(
        fetch_kernel,
        [
            ((thin, 2 * rows), BF16),
            ((thin, rows), BF16),
            ((mix_gain.shape[0] // LANES, LANES), F32),
            (w_query.shape, BF16),
            (w_key.shape, BF16),
            (w_value.shape, BF16),
            ((w_igate.shape[1], LANES), BF16),
            ((w_fgate.shape[1], LANES), BF16),
        ],
        kv_pos,
        tp_pos,
        tokens.T,
        mix_gain.reshape(-1, LANES),
        w_query,
        w_key,
        w_value,
        w_igate.T,
        w_fgate.T,
        scalars=2,
        far=7,
        fetched=6,
        scratch=[pltpu.SemaphoreType.DMA((7,))],
    )
    packed = lax.psum(padded, "tp")

    sends, state_norm, old_stab, ibias, fbias = call(
        project_kernel,
        [
            ((rows, PITCH, LANES), BF16),
            (normalizer.shape[1:], F32),
            (stabilizer.shape, F32),
            ((1, igate_bias.shape[0]), F32),
            ((1, fgate_bias.shape[0]), F32),
        ],
        kv_pos,
        packed,
        gain_near,
        wq,
        wk,
        wv,
        ig,
        fg,
        normalizer[0],
        stabilizer,
        igate_bias[None],
        fgate_bias[None],
        scalars=1,
        far=4,
        fetched=4,
        away=(0,),
        scratch=[pltpu.VMEM((rows * PITCH, LANES), F32), pltpu.SemaphoreType.DMA((4,))],
    )
    arrived = lax.all_to_all(sends, "kv", 0, 0, tiled=True)
    hidden = w_up.shape[1]
    quarter = thin // 2
    gains = mlp_gain.reshape(kv, 2, 2, quarter).transpose(1, 2, 0, 3).reshape(4, kv * quarter)
    keep, send, w_out = call(
        prepare_kernel,
        [((2048, 256), BF16), ((2048, 256), BF16), (w_output.shape[::-1], BF16)],
        tp_pos,
        w_up.reshape(kv, 2, 2, quarter, hidden),
        gains,
        w_down,
        w_output.T,
        scalars=1,
        far=1,
        fetched=1,
        away=(1,),
        scratch=[pltpu.VMEM((kv, 2, 2, quarter, hidden), BF16), pltpu.SemaphoreType.DMA],
    )
    other = lax.ppermute(send, "tp", [(0, 1), (1, 0)])
    arrived, keep, other = lax.optimization_barrier((arrived, keep, other))
    cell, keys, vals, keeps, new_normalizer, new_stabilizer = call(
        cell_kernel,
        [
            ((kv, 16, LANES), BF16),
            ((8, DQK), F32),
            ((8, DV), F32),
            ((8, LANES), F32),
            ((8, DQK), F32),
            ((1, 8), F32),
        ],
        tp_pos,
        arrived,
        state_norm,
        old_stab,
        ibias,
        fbias,
        memory[0],
        scalars=1,
        far=1,
        away=(0, 4, 5),
        scratch=[pltpu.VMEM(memory.shape[1:], F32), pltpu.SemaphoreType.DMA((8,))],
    )
    cells = lax.all_to_all(cell, "kv", 0, 0, tiled=True)
    new_memory = call(
        update_kernel,
        [(memory.shape[1:], F32)],
        keys,
        vals,
        keeps,
        memory[0],
        far=1,
        fetched=1,
        away=(0,),
        scratch=[pltpu.VMEM(memory.shape[1:], F32), pltpu.SemaphoreType.DMA((16,))],
    )

    cells, new_memory = lax.optimization_barrier((cells, new_memory))

    half, crossing = call(
        output_kernel,
        [((quarter, 2 * rows), BF16), ((thin, 2 * rows), BF16)],
        tp_pos,
        cells,
        w_out,
        scalars=1,
        scratch=[pltpu.VMEM((rows * 16, LANES), F32)],
    )
    middle, own = call(
        middle_kernel,
        [((kv, quarter, 2 * rows), BF16), ((quarter, 2 * rows), BF16)],
        tp_pos,
        half,
        lax.psum(crossing, "tp"),
        own_tokens,
        scalars=1,
    )
    middles = lax.all_to_all(middle, "kv", 0, 0, tiled=True).reshape(kv * quarter, 2 * rows)
    sums = call(up_kernel, [((136, 128), F32)], tp_pos, middles, keep, other, scalars=1)
    downs = call(
        down_kernel,
        [((kv * quarter, 2 * rows), BF16)],
        tp_pos,
        sums,
        lax.ppermute(sums, "tp", [(0, 1), (1, 0)]),
        keep,
        other,
        scalars=1,
    )
    back = lax.all_to_all(downs.reshape(kv, quarter, 2 * rows), "kv", 0, 0, tiled=True)
    new_tokens = call(finish_kernel, [((thin, rows), BF16)], back, own, away=(0,)).T
    return (new_tokens, new_memory[None], new_normalizer[None], new_stabilizer)


def solution(mesh):
    in_specs = (
        P("dp", ("kv", "tp")),
        P(),
        P("kv", "tp"),
        P("kv", "tp"),
        P("kv", "tp"),
        P(),
        P(),
        P(),
        P(),
        P(("dp", "kv"), "tp", None, None),
        P(("dp", "kv"), "tp", None),
        P(("dp", "kv"), "tp"),
        P("tp", "kv"),
        P(),
        P(None, ("kv", "tp")),
        P(("kv", "tp"), None),
    )
    out_specs = (
        P("dp", ("kv", "tp")),
        P(("dp", "kv"), "tp", None, None),
        P(("dp", "kv"), "tp", None),
        P(("dp", "kv"), "tp"),
    )
    return jax.shard_map(on_device, mesh=mesh, in_specs=in_specs, out_specs=out_specs, check_vma=False)
```

```python
import jax
import jax.numpy as jnp
from jax import lax
from jax.experimental import pallas as pl
from jax.experimental.pallas import tpu as pltpu
from jax.sharding import PartitionSpec as P


DV = 256
DQK = 128
LANES = 128
NORM_EPS = 1e-06
STACK = 34

F32 = jnp.float32
BF16 = jnp.bfloat16

NT = (((1,), (1,)), ((), ()))

TN = (((0,), (0,)), ((), ()))


def split(wide):
    high = wide.astype(BF16)
    return high, (wide - high.astype(F32)).astype(BF16)


vmem = pl.BlockSpec(memory_space=pltpu.VMEM)
smem = pl.BlockSpec(memory_space=pltpu.SMEM)


any_space = pl.BlockSpec(memory_space=pl.ANY)


def fetch_kernel(kv_pos, tp_pos, tokens, gain, wq, wk, wv, wig, wfg, padded, *rest):
    outs, sems = rest[:-1], rest[-1]
    start = pl.multiple_of(kv_pos[0] // 2 * LANES, LANES)
    sources = (tokens, gain, wq, wk, wv, wig.at[:, pl.ds(start, LANES)], wfg.at[:, pl.ds(start, LANES)])
    copies = [pltpu.make_async_copy(src, dst, sems.at[i]) for i, (src, dst) in enumerate(zip(sources, outs))]
    for copy in copies:
        copy.start()
    copies[0].wait()
    x = outs[0][...].astype(F32)
    twice = jnp.concatenate([x, x], axis=1)
    padded[...] = jnp.where(halves_of(twice) == tp_pos[0], twice, 0.0).astype(BF16)
    for copy in copies[1:]:
        copy.wait()


def project_kernel(kv_pos, packed, gain, wq, wk, wv, wig, wfg, *rest):
    sources, out, held, rows, sems = rest[:4], rest[4], rest[5:9], rest[9], rest[10]
    copies = [pltpu.make_async_copy(src, dst, sems.at[i]) for i, (src, dst) in enumerate(zip(sources, held))]
    for copy in copies:
        copy.start()
    n = packed.shape[1] // 2
    block = kv_pos[0] // 2
    odd = kv_pos[0] % 2
    wide = packed[...].astype(F32)
    x = jnp.concatenate([wide[:, :n].T, wide[:, n:].T], axis=1)
    twice = jnp.concatenate([x, x], axis=1)

    def put(at, tile):
        rows[pl.ds(at // 2 * 2 * n + at % 2, n, stride=2), :] = tile

    lane = lax.broadcasted_iota(jnp.int32, twice.shape, 1)
    mine = (lane // n) == odd
    scaled = jnp.where(mine, twice * gain[pl.ds(block, 1), :], 0.0)
    wide_lhs = scaled.astype(BF16)
    folded = scaled[:, :n] + scaled[:, n:]
    lhs = folded.astype(BF16)
    ig = wig[...]
    fg = wfg[...]
    gates = jnp.concatenate([ig, fg, ig, fg, jnp.zeros((LANES - 4 * ig.shape[0], LANES), BF16)], axis=0)
    sums = lax.dot_general(wide_lhs, gates, NT, preferred_element_type=F32)
    squares = jnp.sum(x * x, axis=1, keepdims=True)
    sums = jnp.where(lane >= n, jnp.broadcast_to(squares, sums.shape), sums)
    low = ((lane >= n // 2) & (lane < n)) | (lane == n + 1)
    sums = jnp.where(low, sums - sums.astype(BF16).astype(F32), sums)
    for at in range(32, STACK):
        put(at, sums)

    def place(w, first, step):
        cols = w.shape[1]
        for c in range(0, cols, 256):
            part = jnp.dot(lhs, w[:, c : c + 256], preferred_element_type=F32)
            for half in range(2):
                tile = c // LANES + half
                at = first + (tile if step == 1 else (tile % 2) * 8 + tile // 2)
                put(at, part[:, half * LANES : (half + 1) * LANES])

    place(wq, 0, 1)
    place(wk, 8, 1)
    place(wv, 16, 2)
    for pair in range(STACK // 2):
        part = rows[pair * 2 * n : (pair + 1) * 2 * n, :].astype(BF16)
        out[:, :, pair * LANES : (pair + 1) * LANES] = part.reshape(n, 2, LANES)
    for copy in copies:
        copy.wait()


def hold_kernel(memory, after, out, sem):
    copy = pltpu.make_async_copy(memory, out, sem)
    copy.start()
    copy.wait()


def cell_kernel(tp_pos, arrived, memory, normalizer, stab, ibias, fbias, out, keys, vals, keeps, norm_out, stab_out):
    tp = tp_pos[0]
    heads = memory.shape[0]
    pad = jnp.zeros((1, LANES - 32), F32)
    bias = jnp.concatenate([ibias[...], fbias[...], pad], axis=1)
    old_stab = jnp.concatenate([stab[...], jnp.zeros((1, LANES - 8), F32)], axis=1)
    count = arrived.shape[0]

    def add(i, acc):
        for j in range(8):
            acc = acc + arrived[i * 8 + j].astype(F32)
        return acc

    acc = lax.fori_loop(0, count // 8, add, jnp.zeros(arrived.shape[1:], F32))

    def stack(first):
        return jnp.concatenate([acc[:, j * LANES : (j + 1) * LANES] for j in range(first // 2, first // 2 + 4)], axis=0)

    lane = lax.broadcasted_iota(jnp.int32, (8, LANES), 1)
    sub = lax.broadcasted_iota(jnp.int32, (8, LANES), 0)
    extra = jnp.broadcast_to(acc[0:1, 16 * LANES :], (8, LANES))
    squares = jnp.sum(jnp.where((lane == 64) | (lane == 65), extra, 0.0), axis=1, keepdims=True)
    scale = lax.rsqrt(squares * (1.0 / 4096.0) + NORM_EPS)
    gates = extra * scale + bias
    head = tp * 8 + sub
    igate = jnp.sum(jnp.where((lane == head) | (lane == head + 32), gates, 0.0), axis=1, keepdims=True)
    fgate = jnp.sum(jnp.where((lane == head + 16) | (lane == head + 48), gates, 0.0), axis=1, keepdims=True)
    old = jnp.sum(jnp.where(lane == sub, old_stab, 0.0), axis=1, keepdims=True)
    log_forget = jnp.minimum(fgate, 0.0) - jnp.log1p(jnp.exp(-jnp.abs(fgate)))
    carried = log_forget + old
    new = jnp.maximum(carried, igate)
    keep = jnp.exp(carried - new)
    fresh = jnp.exp(igate - new)
    stab_out[...] = jnp.sum(jnp.where(lane == sub, new, 0.0), axis=0, keepdims=True)[:, :8]
    q = stack(0) * (scale * DQK ** (-0.5))
    k = stack(8) * scale
    v = jnp.concatenate([stack(16), stack(24)], axis=1) * scale
    q_both = jnp.concatenate(split(q), axis=0)
    sub2 = lax.broadcasted_iota(jnp.int32, (8, DV), 0)
    recall = jnp.zeros((8, DV), F32)
    for h in range(heads):
        part = lax.dot_general(q_both, memory[h].astype(BF16), NT, preferred_element_type=F32)
        recall = jnp.where(sub2 == h, part[:8] + part[8:], recall)
    match = jnp.sum(q * k, axis=1, keepdims=True)
    old_norm = normalizer[...]
    denominator = keep * jnp.sum(old_norm * q, axis=1, keepdims=True) + fresh * match
    floor = jnp.maximum(jnp.abs(denominator), jnp.exp(-new))
    cell = (keep * recall + (fresh * match) * v) / floor
    tile = jnp.concatenate([cell[:, :LANES], cell[:, LANES:]], axis=0).astype(BF16)
    for r in range(count):
        out[r] = tile
    norm_out[...] = keep * old_norm + fresh * k
    keys[...] = k
    vals[...] = fresh * v
    keeps[...] = jnp.broadcast_to(keep, keeps.shape)


def update_kernel(keys, vals, keeps, memory_in, memory_out, memory, sems):
    heads = memory.shape[0]
    loads = [pltpu.make_async_copy(memory_in.at[h], memory.at[h], sems.at[h]) for h in range(heads)]
    stores = [pltpu.make_async_copy(memory.at[h], memory_out.at[h], sems.at[heads + h]) for h in range(heads)]
    for load in loads:
        load.start()
    v_high, v_low = split(vals[...])
    k_high, k_low = split(keys[...])
    for h in range(heads):
        row = slice(h, h + 1)
        left = jnp.concatenate([v_high[row], v_high[row], v_low[row]], axis=0)
        right = jnp.concatenate([k_high[row], k_low[row], k_high[row]], axis=0)
        outer = lax.dot_general(left, right, TN, preferred_element_type=F32)
        loads[h].wait()
        memory[h] = keeps[row, :] * memory[h] + outer
        stores[h].start()
    for store in stores:
        store.wait()


def folded(wide):
    thin = wide.shape[0] // 2
    return jnp.concatenate([wide[:thin], wide[thin:]], axis=1)


def output_kernel(tp_pos, arrived, w, own, out, rows):
    tp = tp_pos[0]
    count = arrived.shape[0]
    for r in range(count):
        rows[r * 16 : r * 16 + 16, :] = arrived[r].astype(F32)
    parts = []
    for tile in range(16):
        c = (tile % 2) * 8 + tile // 2
        parts.append(rows[pl.ds(c, count, stride=16), :].astype(BF16))
    acc = lax.dot_general(w[...], jnp.concatenate(parts, axis=1), NT, preferred_element_type=F32)
    half = acc.shape[0] // 2
    first = folded(acc[:half])
    second = folded(acc[half:])
    own[...] = jnp.where(tp == 0, first, second).astype(BF16)
    out[...] = jnp.concatenate([jnp.where(tp == 1, first, 0.0), jnp.where(tp == 0, second, 0.0)], axis=0).astype(BF16)


def prepare_kernel(tp_pos, w_up, gain, w_down, w_out, keep, send, held, turned, sem):
    copy = pltpu.make_async_copy(w_out, held, sem)
    copy.start()
    tp = tp_pos[0]
    chips = w_up.shape[0]
    for k in range(0, chips, 2):
        turned[k : k + 2] = w_down[:, k * 64 : k * 64 + 128].T.reshape(2, 2, 2, 16, 128)
    for side in range(2):
        dst = (keep, send)[side]
        half = (tp + side) % 2
        for quarter in range(2):
            lanes = slice(quarter * 128, quarter * 128 + 128)
            factors = gain[pl.ds(half * 2 + quarter, 1), :]
            for block in range(4):
                part = w_up[block * 16 : block * 16 + 16, half, quarter].reshape(256, 128).T
                part = part.astype(F32) * factors[:, block * 256 : block * 256 + 256]
                dst[block * 256 + quarter * 128 : block * 256 + quarter * 128 + 128, :] = part.astype(BF16)
            dst[1024:2048, lanes] = turned[:, half, quarter].reshape(1024, 128)
    copy.wait()


def middle_kernel(tp_pos, half, both, tokens, out, own):
    tp = tp_pos[0]
    thin = half.shape[0]
    other = jnp.where(tp == 0, both[:thin].astype(F32), both[thin:].astype(F32))
    tile = (folded(tokens[...].astype(F32)) + half[...].astype(F32) + other).astype(BF16)
    own[...] = tile
    for r in range(out.shape[0]):
        out[r] = tile


def halves_of(like):
    return (lax.broadcasted_iota(jnp.int32, like.shape, 1) >= like.shape[1] // 2).astype(jnp.int32)


def swapped(wide):
    n = wide.shape[1] // 2
    return jnp.concatenate([wide[:, n:], wide[:, :n]], axis=1)


def up_kernel(tp_pos, middle, keep, other, out):
    tp = tp_pos[0]
    wide = middle[...].astype(F32)
    squares = jnp.sum(wide * wide, axis=0, keepdims=True)

    def product(w):
        acc = jnp.zeros((256, 128), F32)
        for block in range(4):
            rows = slice(block * 256, block * 256 + 256)
            acc = acc + jnp.dot(w[rows, :], middle[rows, :], preferred_element_type=F32)
        low = acc[:128] + swapped(acc[128:])
        return jnp.where(halves_of(low) == 0, low, swapped(low))

    own = product(keep)
    out[:128] = jnp.where(halves_of(own) == tp, own, product(other))
    out[128:] = jnp.broadcast_to(squares + swapped(squares), (8, 128))


def down_kernel(tp_pos, near, far_sums, keep, other, out):
    tp = tp_pos[0]
    sums = near[...] + far_sums[...]
    scale = lax.rsqrt(sums[128:129] * (1.0 / 4096.0) + NORM_EPS)
    act = jnp.square(jnp.maximum(sums[:128] * scale, 0.0))
    swap = swapped(act)
    side = halves_of(act)

    def spread(rows):
        return jnp.concatenate([jnp.where(side == 0, rows, 0.0), jnp.where(side == 1, rows, 0.0)], axis=0).astype(BF16)

    own = spread(jnp.where(side == tp, act, swap))
    far = spread(jnp.where(side == tp, swap, act))
    for i in range(0, 1024, 256):
        rows = slice(1024 + i, 1280 + i)
        part = jnp.dot(keep[rows, :], own, preferred_element_type=F32)
        part = part + jnp.dot(other[rows, :], far, preferred_element_type=F32)
        out[i : i + 256, :] = part.astype(BF16)


def finish_kernel(back, own, out):
    def add(i, acc):
        for j in range(8):
            acc = acc + back[i * 8 + j].astype(F32)
        return acc

    acc = lax.fori_loop(0, back.shape[0] // 8, add, own[...].astype(F32))
    n = acc.shape[1] // 2
    out[...] = jnp.concatenate([acc[:, :n], acc[:, n:]], axis=0).astype(BF16)


def call(kernel, shapes, *args, scalars=0, far=0, fetched=0, away=(), scratch=()):
    outs = [pltpu.HBM(s, d) if i in away else pltpu.VMEM(s, d) for i, (s, d) in enumerate(shapes)]
    out_specs = [vmem] * (len(outs) - fetched) + [any_space] * fetched
    many = len(outs) > 1
    near = len(args) - far
    args = args[:near] + tuple(pltpu.with_memory_space_constraint(x, pltpu.HBM) for x in args[near:])
    return pl.pallas_call(
        kernel,
        out_shape=outs if many else outs[0],
        in_specs=[smem] * scalars + [vmem] * (near - scalars) + [any_space] * far,
        out_specs=out_specs if many else out_specs[0],
        scratch_shapes=list(scratch),
        compiler_params=pltpu.CompilerParams(vmem_limit_bytes=16 * 1024 * 1024),
    )(*args)


def on_device(
    tokens,
    mix_gain,
    w_query,
    w_key,
    w_value,
    w_igate,
    w_fgate,
    igate_bias,
    fgate_bias,
    memory,
    normalizer,
    stabilizer,
    w_output,
    mlp_gain,
    w_up,
    w_down,
):
    kv = lax.axis_size("kv")
    kv_index = lax.axis_index("kv")
    tp_index = lax.axis_index("tp")
    rows, thin = tokens.shape
    kv_pos = kv_index.astype(jnp.int32).reshape(1)
    tp_pos = tp_index.astype(jnp.int32).reshape(1)
    padded, own_tokens, gain_near, wq, wk, wv, ig, fg = call(
        fetch_kernel,
        [
            ((thin, 2 * rows), BF16),
            ((thin, rows), BF16),
            ((mix_gain.shape[0] // LANES, LANES), F32),
            (w_query.shape, BF16),
            (w_key.shape, BF16),
            (w_value.shape, BF16),
            ((w_igate.shape[1], LANES), BF16),
            ((w_fgate.shape[1], LANES), BF16),
        ],
        kv_pos,
        tp_pos,
        tokens.T,
        mix_gain.reshape(-1, LANES),
        w_query,
        w_key,
        w_value,
        w_igate.T,
        w_fgate.T,
        scalars=2,
        far=7,
        fetched=6,
        scratch=[pltpu.SemaphoreType.DMA((7,))],
    )
    packed = lax.psum(padded, "tp")

    sends, state_norm, old_stab, ibias, fbias = call(
        project_kernel,
        [
            ((rows, 2, STACK // 2 * LANES), BF16),
            (normalizer.shape[1:], F32),
            (stabilizer.shape, F32),
            ((1, igate_bias.shape[0]), F32),
            ((1, fgate_bias.shape[0]), F32),
        ],
        kv_pos,
        packed,
        gain_near,
        wq,
        wk,
        wv,
        ig,
        fg,
        normalizer[0],
        stabilizer,
        igate_bias[None],
        fgate_bias[None],
        scalars=1,
        far=4,
        fetched=4,
        away=(0,),
        scratch=[pltpu.VMEM((rows * STACK, LANES), F32), pltpu.SemaphoreType.DMA((4,))],
    )
    arrived = lax.all_to_all(sends, "kv", 0, 0, tiled=True)
    hidden = w_up.shape[1]
    quarter = thin // 2
    gains = mlp_gain.reshape(kv, 2, 2, quarter).transpose(1, 2, 0, 3).reshape(4, kv * quarter)
    keep, send, w_out = call(
        prepare_kernel,
        [((2048, 256), BF16), ((2048, 256), BF16), (w_output.shape[::-1], BF16)],
        tp_pos,
        w_up.reshape(kv, 2, 2, quarter, hidden),
        gains,
        w_down,
        w_output.T,
        scalars=1,
        far=1,
        fetched=1,
        away=(0, 1),
        scratch=[pltpu.VMEM((kv, 2, 2, quarter, hidden), BF16), pltpu.SemaphoreType.DMA],
    )
    other = lax.ppermute(send, "tp", [(0, 1), (1, 0)])
    state = pl.pallas_call(
        hold_kernel,
        out_shape=pltpu.VMEM(memory.shape[1:], F32),
        in_specs=[any_space, any_space],
        out_specs=any_space,
        scratch_shapes=[pltpu.SemaphoreType.DMA],
        compiler_params=pltpu.CompilerParams(vmem_limit_bytes=1024 * 1024),
    )(pltpu.with_memory_space_constraint(memory[0], pltpu.HBM), other)
    arrived, keep, other, state = lax.optimization_barrier((arrived, keep, other, state))
    cell, keys, vals, keeps, new_normalizer, new_stabilizer = call(
        cell_kernel,
        [
            ((kv, 16, LANES), BF16),
            ((8, DQK), F32),
            ((8, DV), F32),
            ((8, LANES), F32),
            ((8, DQK), F32),
            ((1, 8), F32),
        ],
        tp_pos,
        arrived,
        state,
        state_norm,
        old_stab,
        ibias,
        fbias,
        scalars=1,
        away=(0, 4, 5),
    )
    cells = lax.all_to_all(cell, "kv", 0, 0, tiled=True)
    new_memory = call(
        update_kernel,
        [(memory.shape[1:], F32)],
        keys,
        vals,
        keeps,
        memory[0],
        far=1,
        fetched=1,
        away=(0,),
        scratch=[pltpu.VMEM(memory.shape[1:], F32), pltpu.SemaphoreType.DMA((16,))],
    )

    cells, new_memory = lax.optimization_barrier((cells, new_memory))

    half, crossing = call(
        output_kernel,
        [((quarter, 2 * rows), BF16), ((thin, 2 * rows), BF16)],
        tp_pos,
        cells,
        w_out,
        scalars=1,
        scratch=[pltpu.VMEM((rows * 16, LANES), F32)],
    )
    middle, own = call(
        middle_kernel,
        [((kv, quarter, 2 * rows), BF16), ((quarter, 2 * rows), BF16)],
        tp_pos,
        half,
        lax.psum(crossing, "tp"),
        own_tokens,
        scalars=1,
    )
    middles = lax.all_to_all(middle, "kv", 0, 0, tiled=True).reshape(kv * quarter, 2 * rows)
    sums = call(up_kernel, [((136, 128), F32)], tp_pos, middles, keep, other, scalars=1)
    downs = call(
        down_kernel,
        [((kv * quarter, 2 * rows), BF16)],
        tp_pos,
        sums,
        lax.ppermute(sums, "tp", [(0, 1), (1, 0)]),
        keep,
        other,
        scalars=1,
    )
    back = lax.all_to_all(downs.reshape(kv, quarter, 2 * rows), "kv", 0, 0, tiled=True)
    new_tokens = call(finish_kernel, [((thin, rows), BF16)], back, own, away=(0,)).T
    return (new_tokens, new_memory[None], new_normalizer[None], new_stabilizer)


def solution(mesh):
    in_specs = (
        P("dp", ("kv", "tp")),
        P(),
        P("kv", "tp"),
        P("kv", "tp"),
        P("kv", "tp"),
        P(),
        P(),
        P(),
        P(),
        P(("dp", "kv"), "tp", None, None),
        P(("dp", "kv"), "tp", None),
        P(("dp", "kv"), "tp"),
        P("tp", "kv"),
        P(),
        P(None, ("kv", "tp")),
        P(("kv", "tp"), None),
    )
    out_specs = (
        P("dp", ("kv", "tp")),
        P(("dp", "kv"), "tp", None, None),
        P(("dp", "kv"), "tp", None),
        P(("dp", "kv"), "tp"),
    )
    return jax.shard_map(on_device, mesh=mesh, in_specs=in_specs, out_specs=out_specs, check_vma=False)
```

```python
import jax
import jax.numpy as jnp
from jax import lax
from jax.experimental import pallas as pl
from jax.experimental.pallas import tpu as pltpu
from jax.sharding import PartitionSpec as P


DV = 256
DQK = 128
LANES = 128
NORM_EPS = 1e-06
STACK = 34

F32 = jnp.float32
BF16 = jnp.bfloat16

NT = (((1,), (1,)), ((), ()))

TN = (((0,), (0,)), ((), ()))


def split(wide):
    high = wide.astype(BF16)
    return high, (wide - high.astype(F32)).astype(BF16)


vmem = pl.BlockSpec(memory_space=pltpu.VMEM)
smem = pl.BlockSpec(memory_space=pltpu.SMEM)


any_space = pl.BlockSpec(memory_space=pl.ANY)


def fetch_kernel(kv_pos, tp_pos, tokens, gain, wq, wk, wv, wig, wfg, padded, *rest):
    outs, sems = rest[:-1], rest[-1]
    start = pl.multiple_of(kv_pos[0] // 2 * LANES, LANES)
    sources = (tokens, gain, wq, wk, wv, wig.at[:, pl.ds(start, LANES)], wfg.at[:, pl.ds(start, LANES)])
    copies = [pltpu.make_async_copy(src, dst, sems.at[i]) for i, (src, dst) in enumerate(zip(sources, outs))]
    for copy in copies:
        copy.start()
    copies[0].wait()
    x = outs[0][...].astype(F32)
    twice = jnp.concatenate([x, x], axis=1)
    padded[...] = jnp.where(halves_of(twice) == tp_pos[0], twice, 0.0).astype(BF16)
    for copy in copies[1:]:
        copy.wait()


def project_kernel(kv_pos, packed, gain, wq, wk, wv, wig, wfg, *rest):
    sources, held, out, rows, ready, sems = rest[:4], rest[4:8], rest[8], rest[9], rest[10], rest[11]
    copies = [pltpu.make_async_copy(src, dst, sems.at[i]) for i, (src, dst) in enumerate(zip(sources, held))]
    for copy in copies:
        copy.start()
    n = packed.shape[1] // 2
    block = kv_pos[0] // 2
    odd = kv_pos[0] % 2
    wide = packed[...].astype(F32)
    x = jnp.concatenate([wide[:, :n].T, wide[:, n:].T], axis=1)
    twice = jnp.concatenate([x, x], axis=1)

    def put(at, tile):
        rows[pl.ds(at // 2 * 2 * n + at % 2, n, stride=2), :] = tile

    lane = lax.broadcasted_iota(jnp.int32, twice.shape, 1)
    mine = (lane // n) == odd
    scaled = jnp.where(mine, twice * gain[pl.ds(block, 1), :], 0.0)
    wide_lhs = scaled.astype(BF16)
    folded = scaled[:, :n] + scaled[:, n:]
    lhs = folded.astype(BF16)
    ig = wig[...]
    fg = wfg[...]
    gates = jnp.concatenate([ig, fg, ig, fg, jnp.zeros((LANES - 4 * ig.shape[0], LANES), BF16)], axis=0)
    sums = lax.dot_general(wide_lhs, gates, NT, preferred_element_type=F32)
    squares = jnp.sum(x * x, axis=1, keepdims=True)
    sums = jnp.where(lane >= n, jnp.broadcast_to(squares, sums.shape), sums)
    low = ((lane >= n // 2) & (lane < n)) | (lane == n + 1)
    sums = jnp.where(low, sums - sums.astype(BF16).astype(F32), sums)
    for at in range(32, STACK):
        put(at, sums)

    def send(first, pairs):
        for pair in range(first, first + pairs):
            part = rows[pair * 2 * n : (pair + 1) * 2 * n, :].astype(BF16)
            ready[:, :, pair * LANES : (pair + 1) * LANES] = part.reshape(n, 2, LANES)
        lanes = pl.ds(first * LANES, pairs * LANES)
        copy = pltpu.make_async_copy(ready.at[:, :, lanes], out.at[:, :, lanes], sems.at[len(copies)])
        copy.start()
        copies.append(copy)

    def place(w, first, start, stop, step):
        for c in range(start, stop, 256):
            part = jnp.dot(lhs, w[:, c : c + 256], preferred_element_type=F32)
            for half in range(2):
                tile = c // LANES + half
                at = first + (tile if step == 1 else (tile % 2) * 8 + tile // 2)
                put(at, part[:, half * LANES : (half + 1) * LANES])

    cols = wq.shape[1]
    place(wq, 0, 0, cols, 1)
    send(0, 4)
    place(wk, 8, 0, cols, 1)
    send(4, 4)
    send(16, 1)
    place(wv, 16, 0, cols, 2)
    send(8, 2)
    send(12, 2)
    place(wv, 16, cols, 2 * cols, 2)
    send(10, 2)
    send(14, 2)
    for copy in copies:
        copy.wait()


def hold_kernel(memory, after, out, sem):
    copy = pltpu.make_async_copy(memory, out, sem)
    copy.start()
    copy.wait()


def cell_kernel(tp_pos, arrived, memory, normalizer, stab, ibias, fbias, out, keys, vals, keeps, norm_out, stab_out):
    tp = tp_pos[0]
    heads = memory.shape[0]
    pad = jnp.zeros((1, LANES - 32), F32)
    bias = jnp.concatenate([ibias[...], fbias[...], pad], axis=1)
    old_stab = jnp.concatenate([stab[...], jnp.zeros((1, LANES - 8), F32)], axis=1)
    count = arrived.shape[0]

    def add(i, acc):
        for j in range(8):
            acc = acc + arrived[i * 8 + j].astype(F32)
        return acc

    acc = lax.fori_loop(0, count // 8, add, jnp.zeros(arrived.shape[1:], F32))

    def stack(first):
        return jnp.concatenate([acc[:, j * LANES : (j + 1) * LANES] for j in range(first // 2, first // 2 + 4)], axis=0)

    lane = lax.broadcasted_iota(jnp.int32, (8, LANES), 1)
    sub = lax.broadcasted_iota(jnp.int32, (8, LANES), 0)
    extra = jnp.broadcast_to(acc[0:1, 16 * LANES :], (8, LANES))
    squares = jnp.sum(jnp.where((lane == 64) | (lane == 65), extra, 0.0), axis=1, keepdims=True)
    scale = lax.rsqrt(squares * (1.0 / 4096.0) + NORM_EPS)
    gates = extra * scale + bias
    head = tp * 8 + sub
    igate = jnp.sum(jnp.where((lane == head) | (lane == head + 32), gates, 0.0), axis=1, keepdims=True)
    fgate = jnp.sum(jnp.where((lane == head + 16) | (lane == head + 48), gates, 0.0), axis=1, keepdims=True)
    old = jnp.sum(jnp.where(lane == sub, old_stab, 0.0), axis=1, keepdims=True)
    log_forget = jnp.minimum(fgate, 0.0) - jnp.log1p(jnp.exp(-jnp.abs(fgate)))
    carried = log_forget + old
    new = jnp.maximum(carried, igate)
    keep = jnp.exp(carried - new)
    fresh = jnp.exp(igate - new)
    stab_out[...] = jnp.sum(jnp.where(lane == sub, new, 0.0), axis=0, keepdims=True)[:, :8]
    q = stack(0) * (scale * DQK ** (-0.5))
    k = stack(8) * scale
    v = jnp.concatenate([stack(16), stack(24)], axis=1) * scale
    q_both = jnp.concatenate(split(q), axis=0)
    sub2 = lax.broadcasted_iota(jnp.int32, (8, DV), 0)
    recall = jnp.zeros((8, DV), F32)
    for h in range(heads):
        part = lax.dot_general(q_both, memory[h].astype(BF16), NT, preferred_element_type=F32)
        recall = jnp.where(sub2 == h, part[:8] + part[8:], recall)
    match = jnp.sum(q * k, axis=1, keepdims=True)
    old_norm = normalizer[...]
    denominator = keep * jnp.sum(old_norm * q, axis=1, keepdims=True) + fresh * match
    floor = jnp.maximum(jnp.abs(denominator), jnp.exp(-new))
    cell = (keep * recall + (fresh * match) * v) / floor
    tile = jnp.concatenate([cell[:, :LANES], cell[:, LANES:]], axis=0).astype(BF16)
    for r in range(count):
        out[r] = tile
    norm_out[...] = keep * old_norm + fresh * k
    keys[...] = k
    vals[...] = fresh * v
    keeps[...] = jnp.broadcast_to(keep, keeps.shape)


def update_kernel(keys, vals, keeps, memory, memory_out, fresh, sems):
    heads = memory.shape[0]
    stores = [pltpu.make_async_copy(fresh.at[h], memory_out.at[h], sems.at[h]) for h in range(heads)]
    v_high, v_low = split(vals[...])
    k_high, k_low = split(keys[...])
    for h in range(heads):
        row = slice(h, h + 1)
        left = jnp.concatenate([v_high[row], v_high[row], v_low[row]], axis=0)
        right = jnp.concatenate([k_high[row], k_low[row], k_high[row]], axis=0)
        outer = lax.dot_general(left, right, TN, preferred_element_type=F32)
        fresh[h] = keeps[row, :] * memory[h] + outer
        stores[h].start()
    for store in stores:
        store.wait()


def folded(wide):
    thin = wide.shape[0] // 2
    return jnp.concatenate([wide[:thin], wide[thin:]], axis=1)


def output_kernel(tp_pos, arrived, w, own, out, rows):
    tp = tp_pos[0]
    count = arrived.shape[0]
    for r in range(count):
        rows[r * 16 : r * 16 + 16, :] = arrived[r].astype(F32)
    parts = []
    for tile in range(16):
        c = (tile % 2) * 8 + tile // 2
        parts.append(rows[pl.ds(c, count, stride=16), :].astype(BF16))
    acc = lax.dot_general(w[...], jnp.concatenate(parts, axis=1), NT, preferred_element_type=F32)
    half = acc.shape[0] // 2
    first = folded(acc[:half])
    second = folded(acc[half:])
    own[...] = jnp.where(tp == 0, first, second).astype(BF16)
    out[...] = jnp.concatenate([jnp.where(tp == 1, first, 0.0), jnp.where(tp == 0, second, 0.0)], axis=0).astype(BF16)


def prepare_kernel(tp_pos, w_up, gain, w_down, w_out, keep, send, held, turned, sem):
    copy = pltpu.make_async_copy(w_out, held, sem)
    copy.start()
    tp = tp_pos[0]
    chips = w_up.shape[0]
    for k in range(0, chips, 2):
        turned[k : k + 2] = w_down[:, k * 64 : k * 64 + 128].T.reshape(2, 2, 2, 16, 128)
    for side in range(2):
        dst = (keep, send)[side]
        half = (tp + side) % 2
        for quarter in range(2):
            lanes = slice(quarter * 128, quarter * 128 + 128)
            factors = gain[pl.ds(half * 2 + quarter, 1), :]
            for block in range(4):
                part = w_up[block * 16 : block * 16 + 16, half, quarter].reshape(256, 128).T
                part = part.astype(F32) * factors[:, block * 256 : block * 256 + 256]
                dst[block * 256 + quarter * 128 : block * 256 + quarter * 128 + 128, :] = part.astype(BF16)
            dst[1024:2048, lanes] = turned[:, half, quarter].reshape(1024, 128)
    copy.wait()


def middle_kernel(tp_pos, half, both, tokens, out, own):
    tp = tp_pos[0]
    thin = half.shape[0]
    other = jnp.where(tp == 0, both[:thin].astype(F32), both[thin:].astype(F32))
    tile = (folded(tokens[...].astype(F32)) + half[...].astype(F32) + other).astype(BF16)
    own[...] = tile
    for r in range(out.shape[0]):
        out[r] = tile


def halves_of(like):
    return (lax.broadcasted_iota(jnp.int32, like.shape, 1) >= like.shape[1] // 2).astype(jnp.int32)


def swapped(wide):
    n = wide.shape[1] // 2
    return jnp.concatenate([wide[:, n:], wide[:, :n]], axis=1)


def up_kernel(tp_pos, middle, keep, other, out):
    tp = tp_pos[0]
    wide = middle[...].astype(F32)
    squares = jnp.sum(wide * wide, axis=0, keepdims=True)

    def product(w):
        acc = jnp.zeros((256, 128), F32)
        for block in range(4):
            rows = slice(block * 256, block * 256 + 256)
            acc = acc + jnp.dot(w[rows, :], middle[rows, :], preferred_element_type=F32)
        low = acc[:128] + swapped(acc[128:])
        return jnp.where(halves_of(low) == 0, low, swapped(low))

    own = product(keep)
    out[:128] = jnp.where(halves_of(own) == tp, own, product(other))
    out[128:] = jnp.broadcast_to(squares + swapped(squares), (8, 128))


def down_kernel(tp_pos, near, far_sums, keep, other, out):
    tp = tp_pos[0]
    sums = near[...] + far_sums[...]
    scale = lax.rsqrt(sums[128:129] * (1.0 / 4096.0) + NORM_EPS)
    act = jnp.square(jnp.maximum(sums[:128] * scale, 0.0))
    swap = swapped(act)
    side = halves_of(act)

    def spread(rows):
        return jnp.concatenate([jnp.where(side == 0, rows, 0.0), jnp.where(side == 1, rows, 0.0)], axis=0).astype(BF16)

    own = spread(jnp.where(side == tp, act, swap))
    far = spread(jnp.where(side == tp, swap, act))
    for i in range(0, 1024, 256):
        rows = slice(1024 + i, 1280 + i)
        part = jnp.dot(keep[rows, :], own, preferred_element_type=F32)
        part = part + jnp.dot(other[rows, :], far, preferred_element_type=F32)
        out[i : i + 256, :] = part.astype(BF16)


def finish_kernel(back, own, out):
    def add(i, acc):
        for j in range(8):
            acc = acc + back[i * 8 + j].astype(F32)
        return acc

    acc = lax.fori_loop(0, back.shape[0] // 8, add, own[...].astype(F32))
    n = acc.shape[1] // 2
    out[...] = jnp.concatenate([acc[:, :n], acc[:, n:]], axis=0).astype(BF16)


def call(kernel, shapes, *args, scalars=0, far=0, fetched=0, away=(), scratch=()):
    outs = [pltpu.HBM(s, d) if i in away else pltpu.VMEM(s, d) for i, (s, d) in enumerate(shapes)]
    out_specs = [vmem] * (len(outs) - fetched) + [any_space] * fetched
    many = len(outs) > 1
    near = len(args) - far
    args = args[:near] + tuple(pltpu.with_memory_space_constraint(x, pltpu.HBM) for x in args[near:])
    return pl.pallas_call(
        kernel,
        out_shape=outs if many else outs[0],
        in_specs=[smem] * scalars + [vmem] * (near - scalars) + [any_space] * far,
        out_specs=out_specs if many else out_specs[0],
        scratch_shapes=list(scratch),
        compiler_params=pltpu.CompilerParams(vmem_limit_bytes=16 * 1024 * 1024),
    )(*args)


def on_device(
    tokens,
    mix_gain,
    w_query,
    w_key,
    w_value,
    w_igate,
    w_fgate,
    igate_bias,
    fgate_bias,
    memory,
    normalizer,
    stabilizer,
    w_output,
    mlp_gain,
    w_up,
    w_down,
):
    kv = lax.axis_size("kv")
    kv_index = lax.axis_index("kv")
    tp_index = lax.axis_index("tp")
    rows, thin = tokens.shape
    kv_pos = kv_index.astype(jnp.int32).reshape(1)
    tp_pos = tp_index.astype(jnp.int32).reshape(1)
    padded, own_tokens, gain_near, wq, wk, wv, ig, fg = call(
        fetch_kernel,
        [
            ((thin, 2 * rows), BF16),
            ((thin, rows), BF16),
            ((mix_gain.shape[0] // LANES, LANES), F32),
            (w_query.shape, BF16),
            (w_key.shape, BF16),
            (w_value.shape, BF16),
            ((w_igate.shape[1], LANES), BF16),
            ((w_fgate.shape[1], LANES), BF16),
        ],
        kv_pos,
        tp_pos,
        tokens.T,
        mix_gain.reshape(-1, LANES),
        w_query,
        w_key,
        w_value,
        w_igate.T,
        w_fgate.T,
        scalars=2,
        far=7,
        fetched=6,
        scratch=[pltpu.SemaphoreType.DMA((7,))],
    )
    packed = lax.psum(padded, "tp")

    state_norm, old_stab, ibias, fbias, sends = call(
        project_kernel,
        [
            (normalizer.shape[1:], F32),
            (stabilizer.shape, F32),
            ((1, igate_bias.shape[0]), F32),
            ((1, fgate_bias.shape[0]), F32),
            ((rows, 2, STACK // 2 * LANES), BF16),
        ],
        kv_pos,
        packed,
        gain_near,
        wq,
        wk,
        wv,
        ig,
        fg,
        normalizer[0],
        stabilizer,
        igate_bias[None],
        fgate_bias[None],
        scalars=1,
        far=4,
        fetched=5,
        away=(4,),
        scratch=[
            pltpu.VMEM((rows * STACK, LANES), F32),
            pltpu.VMEM((rows, 2, STACK // 2 * LANES), BF16),
            pltpu.SemaphoreType.DMA((11,)),
        ],
    )
    arrived = lax.all_to_all(sends, "kv", 0, 0, tiled=True)
    hidden = w_up.shape[1]
    quarter = thin // 2
    gains = mlp_gain.reshape(kv, 2, 2, quarter).transpose(1, 2, 0, 3).reshape(4, kv * quarter)
    keep, send, w_out = call(
        prepare_kernel,
        [((2048, 256), BF16), ((2048, 256), BF16), (w_output.shape[::-1], BF16)],
        tp_pos,
        w_up.reshape(kv, 2, 2, quarter, hidden),
        gains,
        w_down,
        w_output.T,
        scalars=1,
        far=1,
        fetched=1,
        away=(0, 1),
        scratch=[pltpu.VMEM((kv, 2, 2, quarter, hidden), BF16), pltpu.SemaphoreType.DMA],
    )
    other = lax.ppermute(send, "tp", [(0, 1), (1, 0)])
    state = pl.pallas_call(
        hold_kernel,
        out_shape=pltpu.VMEM(memory.shape[1:], F32),
        in_specs=[any_space, any_space],
        out_specs=any_space,
        scratch_shapes=[pltpu.SemaphoreType.DMA],
        compiler_params=pltpu.CompilerParams(vmem_limit_bytes=1024 * 1024),
    )(pltpu.with_memory_space_constraint(memory[0], pltpu.HBM), other)
    arrived, keep, other, state = lax.optimization_barrier((arrived, keep, other, state))
    cell, keys, vals, keeps, new_normalizer, new_stabilizer = call(
        cell_kernel,
        [
            ((kv, 16, LANES), BF16),
            ((8, DQK), F32),
            ((8, DV), F32),
            ((8, LANES), F32),
            ((8, DQK), F32),
            ((1, 8), F32),
        ],
        tp_pos,
        arrived,
        state,
        state_norm,
        old_stab,
        ibias,
        fbias,
        scalars=1,
        away=(4, 5),
    )
    cells = lax.all_to_all(cell, "kv", 0, 0, tiled=True)
    half, crossing = call(
        output_kernel,
        [((quarter, 2 * rows), BF16), ((thin, 2 * rows), BF16)],
        tp_pos,
        cells,
        w_out,
        scalars=1,
        scratch=[pltpu.VMEM((rows * 16, LANES), F32)],
    )
    middle, own = call(
        middle_kernel,
        [((kv, quarter, 2 * rows), BF16), ((quarter, 2 * rows), BF16)],
        tp_pos,
        half,
        lax.psum(crossing, "tp"),
        own_tokens,
        scalars=1,
    )
    middles = lax.all_to_all(middle, "kv", 0, 0, tiled=True).reshape(kv * quarter, 2 * rows)
    sums = call(up_kernel, [((136, 128), F32)], tp_pos, middles, keep, other, scalars=1)
    far_sums = lax.ppermute(sums, "tp", [(0, 1), (1, 0)])
    new_memory = call(
        update_kernel,
        [(memory.shape[1:], F32)],
        keys,
        vals,
        keeps,
        state,
        fetched=1,
        away=(0,),
        scratch=[pltpu.VMEM(memory.shape[1:], F32), pltpu.SemaphoreType.DMA((8,))],
    )
    downs = call(
        down_kernel,
        [((kv * quarter, 2 * rows), BF16)],
        tp_pos,
        sums,
        far_sums,
        keep,
        other,
        scalars=1,
    )
    back = lax.all_to_all(downs.reshape(kv, quarter, 2 * rows), "kv", 0, 0, tiled=True)
    new_tokens = call(finish_kernel, [((thin, rows), BF16)], back, own, away=(0,)).T
    return (new_tokens, new_memory[None], new_normalizer[None], new_stabilizer)


def solution(mesh):
    in_specs = (
        P("dp", ("kv", "tp")),
        P(),
        P("kv", "tp"),
        P("kv", "tp"),
        P("kv", "tp"),
        P(),
        P(),
        P(),
        P(),
        P(("dp", "kv"), "tp", None, None),
        P(("dp", "kv"), "tp", None),
        P(("dp", "kv"), "tp"),
        P("tp", "kv"),
        P(),
        P(None, ("kv", "tp")),
        P(("kv", "tp"), None),
    )
    out_specs = (
        P("dp", ("kv", "tp")),
        P(("dp", "kv"), "tp", None, None),
        P(("dp", "kv"), "tp", None),
        P(("dp", "kv"), "tp"),
    )
    return jax.shard_map(on_device, mesh=mesh, in_specs=in_specs, out_specs=out_specs, check_vma=False)
```

```python
import jax
import jax.numpy as jnp
from jax import lax
from jax.experimental import pallas as pl
from jax.experimental.pallas import tpu as pltpu
from jax.sharding import PartitionSpec as P


DV = 256
DQK = 128
LANES = 128
NORM_EPS = 1e-06
STACK = 34

F32 = jnp.float32
BF16 = jnp.bfloat16

NT = (((1,), (1,)), ((), ()))

TN = (((0,), (0,)), ((), ()))


def split(wide):
    high = wide.astype(BF16)
    return high, (wide - high.astype(F32)).astype(BF16)


vmem = pl.BlockSpec(memory_space=pltpu.VMEM)
smem = pl.BlockSpec(memory_space=pltpu.SMEM)


any_space = pl.BlockSpec(memory_space=pl.ANY)


def fetch_kernel(kv_pos, tokens, gain, wq, wk, wv, wig, wfg, *rest):
    outs, sems = rest[:-1], rest[-1]
    start = pl.multiple_of(kv_pos[0] // 2 * LANES, LANES)
    sources = (tokens, gain, wq, wk, wv, wig.at[:, pl.ds(start, LANES)], wfg.at[:, pl.ds(start, LANES)])
    copies = [pltpu.make_async_copy(src, dst, sems.at[i]) for i, (src, dst) in enumerate(zip(sources, outs))]
    for copy in copies:
        copy.start()
    for copy in copies:
        copy.wait()


def project_kernel(kv_pos, tp_pos, own, other, gain, wq, wk, wv, wig, wfg, *rest):
    sources, held, out, rows, ready, sems = rest[:4], rest[4:8], rest[8], rest[9], rest[10], rest[11]
    copies = [pltpu.make_async_copy(src, dst, sems.at[i]) for i, (src, dst) in enumerate(zip(sources, held))]
    for copy in copies:
        copy.start()
    n = own.shape[1]
    block = kv_pos[0] // 2
    odd = kv_pos[0] % 2
    near = own[...].astype(F32)
    far = other[...].astype(F32)
    first = jnp.where(tp_pos[0] == 0, near, far)
    second = jnp.where(tp_pos[0] == 0, far, near)
    x = jnp.concatenate([first.T, second.T], axis=1)
    twice = jnp.concatenate([x, x], axis=1)

    def put(at, tile):
        rows[pl.ds(at // 2 * 2 * n + at % 2, n, stride=2), :] = tile

    lane = lax.broadcasted_iota(jnp.int32, twice.shape, 1)
    mine = (lane // n) == odd
    scaled = jnp.where(mine, twice * gain[pl.ds(block, 1), :], 0.0)
    wide_lhs = scaled.astype(BF16)
    folded = scaled[:, :n] + scaled[:, n:]
    lhs = folded.astype(BF16)
    ig = wig[...]
    fg = wfg[...]
    gates = jnp.concatenate([ig, fg, ig, fg, jnp.zeros((LANES - 4 * ig.shape[0], LANES), BF16)], axis=0)
    sums = lax.dot_general(wide_lhs, gates, NT, preferred_element_type=F32)
    squares = jnp.sum(x * x, axis=1, keepdims=True)
    sums = jnp.where(lane >= n, jnp.broadcast_to(squares, sums.shape), sums)
    low = ((lane >= n // 2) & (lane < n)) | (lane == n + 1)
    sums = jnp.where(low, sums - sums.astype(BF16).astype(F32), sums)
    for at in range(32, STACK):
        put(at, sums)

    def send(first, pairs):
        for pair in range(first, first + pairs):
            part = rows[pair * 2 * n : (pair + 1) * 2 * n, :].astype(BF16)
            ready[:, :, pair * LANES : (pair + 1) * LANES] = part.reshape(n, 2, LANES)
        lanes = pl.ds(first * LANES, pairs * LANES)
        copy = pltpu.make_async_copy(ready.at[:, :, lanes], out.at[:, :, lanes], sems.at[len(copies)])
        copy.start()
        copies.append(copy)

    def place(w, first, start, stop, step):
        for c in range(start, stop, 256):
            part = jnp.dot(lhs, w[:, c : c + 256], preferred_element_type=F32)
            for half in range(2):
                tile = c // LANES + half
                at = first + (tile if step == 1 else (tile % 2) * 8 + tile // 2)
                put(at, part[:, half * LANES : (half + 1) * LANES])

    cols = wq.shape[1]
    place(wq, 0, 0, cols, 1)
    send(0, 4)
    place(wk, 8, 0, cols, 1)
    send(4, 4)
    send(16, 1)
    place(wv, 16, 0, cols, 2)
    send(8, 2)
    send(12, 2)
    place(wv, 16, cols, 2 * cols, 2)
    send(10, 2)
    send(14, 2)
    for copy in copies:
        copy.wait()


def hold_kernel(memory, after, out, sem):
    copy = pltpu.make_async_copy(memory, out, sem)
    copy.start()
    copy.wait()


def cell_kernel(tp_pos, arrived, memory, normalizer, stab, ibias, fbias, out, keys, vals, keeps, norm_out, stab_out):
    tp = tp_pos[0]
    heads = memory.shape[0]
    pad = jnp.zeros((1, LANES - 32), F32)
    bias = jnp.concatenate([ibias[...], fbias[...], pad], axis=1)
    old_stab = jnp.concatenate([stab[...], jnp.zeros((1, LANES - 8), F32)], axis=1)
    count = arrived.shape[0]

    def add(i, acc):
        for j in range(8):
            acc = acc + arrived[i * 8 + j].astype(F32)
        return acc

    acc = lax.fori_loop(0, count // 8, add, jnp.zeros(arrived.shape[1:], F32))

    def stack(first):
        return jnp.concatenate([acc[:, j * LANES : (j + 1) * LANES] for j in range(first // 2, first // 2 + 4)], axis=0)

    lane = lax.broadcasted_iota(jnp.int32, (8, LANES), 1)
    sub = lax.broadcasted_iota(jnp.int32, (8, LANES), 0)
    extra = jnp.broadcast_to(acc[0:1, 16 * LANES :], (8, LANES))
    squares = jnp.sum(jnp.where((lane == 64) | (lane == 65), extra, 0.0), axis=1, keepdims=True)
    scale = lax.rsqrt(squares * (1.0 / 4096.0) + NORM_EPS)
    gates = extra * scale + bias
    head = tp * 8 + sub
    igate = jnp.sum(jnp.where((lane == head) | (lane == head + 32), gates, 0.0), axis=1, keepdims=True)
    fgate = jnp.sum(jnp.where((lane == head + 16) | (lane == head + 48), gates, 0.0), axis=1, keepdims=True)
    old = jnp.sum(jnp.where(lane == sub, old_stab, 0.0), axis=1, keepdims=True)
    log_forget = jnp.minimum(fgate, 0.0) - jnp.log1p(jnp.exp(-jnp.abs(fgate)))
    carried = log_forget + old
    new = jnp.maximum(carried, igate)
    keep = jnp.exp(carried - new)
    fresh = jnp.exp(igate - new)
    stab_out[...] = jnp.sum(jnp.where(lane == sub, new, 0.0), axis=0, keepdims=True)[:, :8]
    q = stack(0) * (scale * DQK ** (-0.5))
    k = stack(8) * scale
    v = jnp.concatenate([stack(16), stack(24)], axis=1) * scale
    q_both = jnp.concatenate(split(q), axis=0)
    sub2 = lax.broadcasted_iota(jnp.int32, (8, DV), 0)
    recall = jnp.zeros((8, DV), F32)
    for h in range(heads):
        part = lax.dot_general(q_both, memory[h].astype(BF16), NT, preferred_element_type=F32)
        recall = jnp.where(sub2 == h, part[:8] + part[8:], recall)
    match = jnp.sum(q * k, axis=1, keepdims=True)
    old_norm = normalizer[...]
    denominator = keep * jnp.sum(old_norm * q, axis=1, keepdims=True) + fresh * match
    floor = jnp.maximum(jnp.abs(denominator), jnp.exp(-new))
    cell = (keep * recall + (fresh * match) * v) / floor
    tile = jnp.concatenate([cell[:, :LANES], cell[:, LANES:]], axis=0).astype(BF16)
    for r in range(count):
        out[r] = tile
    norm_out[...] = keep * old_norm + fresh * k
    keys[...] = k
    vals[...] = fresh * v
    keeps[...] = jnp.broadcast_to(keep, keeps.shape)


def update_kernel(keys, vals, keeps, memory, memory_out, fresh, sems):
    heads = memory.shape[0]
    stores = [pltpu.make_async_copy(fresh.at[h], memory_out.at[h], sems.at[h]) for h in range(heads)]
    v_high, v_low = split(vals[...])
    k_high, k_low = split(keys[...])
    for h in range(heads):
        row = slice(h, h + 1)
        left = jnp.concatenate([v_high[row], v_high[row], v_low[row]], axis=0)
        right = jnp.concatenate([k_high[row], k_low[row], k_high[row]], axis=0)
        outer = lax.dot_general(left, right, TN, preferred_element_type=F32)
        fresh[h] = keeps[row, :] * memory[h] + outer
        stores[h].start()
    for store in stores:
        store.wait()


def folded(wide):
    thin = wide.shape[0] // 2
    return jnp.concatenate([wide[:thin], wide[thin:]], axis=1)


def output_kernel(tp_pos, arrived, w, own, out, rows):
    tp = tp_pos[0]
    count = arrived.shape[0]
    for r in range(count):
        rows[r * 16 : r * 16 + 16, :] = arrived[r].astype(F32)
    parts = []
    for tile in range(16):
        c = (tile % 2) * 8 + tile // 2
        parts.append(rows[pl.ds(c, count, stride=16), :].astype(BF16))
    acc = lax.dot_general(w[...], jnp.concatenate(parts, axis=1), NT, preferred_element_type=F32)
    half = acc.shape[0] // 2
    first = folded(acc[:half])
    second = folded(acc[half:])
    own[...] = jnp.where(tp == 0, first, second).astype(BF16)
    out[...] = jnp.concatenate([jnp.where(tp == 1, first, 0.0), jnp.where(tp == 0, second, 0.0)], axis=0).astype(BF16)


def prepare_kernel(tp_pos, w_up, gain, w_down, w_out, keep, send, held, turned, sem):
    copy = pltpu.make_async_copy(w_out, held, sem)
    copy.start()
    tp = tp_pos[0]
    chips = w_up.shape[0]
    for k in range(0, chips, 2):
        turned[k : k + 2] = w_down[:, k * 64 : k * 64 + 128].T.reshape(2, 2, 2, 16, 128)
    for side in range(2):
        dst = (keep, send)[side]
        half = (tp + side) % 2
        for quarter in range(2):
            lanes = slice(quarter * 128, quarter * 128 + 128)
            factors = gain[pl.ds(half * 2 + quarter, 1), :]
            for block in range(4):
                part = w_up[block * 16 : block * 16 + 16, half, quarter].reshape(256, 128).T
                part = part.astype(F32) * factors[:, block * 256 : block * 256 + 256]
                dst[block * 256 + quarter * 128 : block * 256 + quarter * 128 + 128, :] = part.astype(BF16)
            dst[1024:2048, lanes] = turned[:, half, quarter].reshape(1024, 128)
    copy.wait()


def middle_kernel(tp_pos, half, both, tokens, out, own):
    tp = tp_pos[0]
    thin = half.shape[0]
    other = jnp.where(tp == 0, both[:thin].astype(F32), both[thin:].astype(F32))
    tile = (folded(tokens[...].astype(F32)) + half[...].astype(F32) + other).astype(BF16)
    own[...] = tile
    for r in range(out.shape[0]):
        out[r] = tile


def halves_of(like):
    return (lax.broadcasted_iota(jnp.int32, like.shape, 1) >= like.shape[1] // 2).astype(jnp.int32)


def swapped(wide):
    n = wide.shape[1] // 2
    return jnp.concatenate([wide[:, n:], wide[:, :n]], axis=1)


def up_kernel(tp_pos, middle, keep, other, out):
    tp = tp_pos[0]
    wide = middle[...].astype(F32)
    squares = jnp.sum(wide * wide, axis=0, keepdims=True)

    def product(w):
        acc = jnp.zeros((256, 128), F32)
        for block in range(4):
            rows = slice(block * 256, block * 256 + 256)
            acc = acc + jnp.dot(w[rows, :], middle[rows, :], preferred_element_type=F32)
        low = acc[:128] + swapped(acc[128:])
        return jnp.where(halves_of(low) == 0, low, swapped(low))

    own = product(keep)
    out[:128] = jnp.where(halves_of(own) == tp, own, product(other))
    out[128:] = jnp.broadcast_to(squares + swapped(squares), (8, 128))


def down_kernel(tp_pos, near, far_sums, keep, other, out):
    tp = tp_pos[0]
    sums = near[...] + far_sums[...]
    scale = lax.rsqrt(sums[128:129] * (1.0 / 4096.0) + NORM_EPS)
    act = jnp.square(jnp.maximum(sums[:128] * scale, 0.0))
    swap = swapped(act)
    side = halves_of(act)

    def spread(rows):
        return jnp.concatenate([jnp.where(side == 0, rows, 0.0), jnp.where(side == 1, rows, 0.0)], axis=0).astype(BF16)

    own = spread(jnp.where(side == tp, act, swap))
    far = spread(jnp.where(side == tp, swap, act))
    for i in range(0, 1024, 256):
        rows = slice(1024 + i, 1280 + i)
        part = jnp.dot(keep[rows, :], own, preferred_element_type=F32)
        part = part + jnp.dot(other[rows, :], far, preferred_element_type=F32)
        out[i : i + 256, :] = part.astype(BF16)


def finish_kernel(back, own, out):
    def add(i, acc):
        for j in range(8):
            acc = acc + back[i * 8 + j].astype(F32)
        return acc

    acc = lax.fori_loop(0, back.shape[0] // 8, add, own[...].astype(F32))
    n = acc.shape[1] // 2
    out[...] = jnp.concatenate([acc[:, :n], acc[:, n:]], axis=0).astype(BF16)


def call(kernel, shapes, *args, scalars=0, far=0, fetched=0, away=(), scratch=()):
    outs = [pltpu.HBM(s, d) if i in away else pltpu.VMEM(s, d) for i, (s, d) in enumerate(shapes)]
    out_specs = [vmem] * (len(outs) - fetched) + [any_space] * fetched
    many = len(outs) > 1
    near = len(args) - far
    args = args[:near] + tuple(pltpu.with_memory_space_constraint(x, pltpu.HBM) for x in args[near:])
    return pl.pallas_call(
        kernel,
        out_shape=outs if many else outs[0],
        in_specs=[smem] * scalars + [vmem] * (near - scalars) + [any_space] * far,
        out_specs=out_specs if many else out_specs[0],
        scratch_shapes=list(scratch),
        compiler_params=pltpu.CompilerParams(vmem_limit_bytes=16 * 1024 * 1024),
    )(*args)


def on_device(
    tokens,
    mix_gain,
    w_query,
    w_key,
    w_value,
    w_igate,
    w_fgate,
    igate_bias,
    fgate_bias,
    memory,
    normalizer,
    stabilizer,
    w_output,
    mlp_gain,
    w_up,
    w_down,
):
    kv = lax.axis_size("kv")
    kv_index = lax.axis_index("kv")
    tp_index = lax.axis_index("tp")
    rows, thin = tokens.shape
    kv_pos = kv_index.astype(jnp.int32).reshape(1)
    tp_pos = tp_index.astype(jnp.int32).reshape(1)
    far_tokens = lax.ppermute(tokens.T, "tp", [(0, 1), (1, 0)])
    own_tokens, gain_near, wq, wk, wv, ig, fg = call(
        fetch_kernel,
        [
            ((thin, rows), BF16),
            ((mix_gain.shape[0] // LANES, LANES), F32),
            (w_query.shape, BF16),
            (w_key.shape, BF16),
            (w_value.shape, BF16),
            ((w_igate.shape[1], LANES), BF16),
            ((w_fgate.shape[1], LANES), BF16),
        ],
        kv_pos,
        tokens.T,
        mix_gain.reshape(-1, LANES),
        w_query,
        w_key,
        w_value,
        w_igate.T,
        w_fgate.T,
        scalars=1,
        far=7,
        fetched=7,
        scratch=[pltpu.SemaphoreType.DMA((7,))],
    )

    state_norm, old_stab, ibias, fbias, sends = call(
        project_kernel,
        [
            (normalizer.shape[1:], F32),
            (stabilizer.shape, F32),
            ((1, igate_bias.shape[0]), F32),
            ((1, fgate_bias.shape[0]), F32),
            ((rows, 2, STACK // 2 * LANES), BF16),
        ],
        kv_pos,
        tp_pos,
        own_tokens,
        far_tokens,
        gain_near,
        wq,
        wk,
        wv,
        ig,
        fg,
        normalizer[0],
        stabilizer,
        igate_bias[None],
        fgate_bias[None],
        scalars=2,
        far=4,
        fetched=5,
        away=(4,),
        scratch=[
            pltpu.VMEM((rows * STACK, LANES), F32),
            pltpu.VMEM((rows, 2, STACK // 2 * LANES), BF16),
            pltpu.SemaphoreType.DMA((11,)),
        ],
    )
    arrived = lax.all_to_all(sends, "kv", 0, 0, tiled=True)
    hidden = w_up.shape[1]
    quarter = thin // 2
    gains = mlp_gain.reshape(kv, 2, 2, quarter).transpose(1, 2, 0, 3).reshape(4, kv * quarter)
    keep, send, w_out = call(
        prepare_kernel,
        [((2048, 256), BF16), ((2048, 256), BF16), (w_output.shape[::-1], BF16)],
        tp_pos,
        w_up.reshape(kv, 2, 2, quarter, hidden),
        gains,
        w_down,
        w_output.T,
        scalars=1,
        far=1,
        fetched=1,
        away=(0, 1),
        scratch=[pltpu.VMEM((kv, 2, 2, quarter, hidden), BF16), pltpu.SemaphoreType.DMA],
    )
    other = lax.ppermute(send, "tp", [(0, 1), (1, 0)])
    state = pl.pallas_call(
        hold_kernel,
        out_shape=pltpu.VMEM(memory.shape[1:], F32),
        in_specs=[any_space, any_space],
        out_specs=any_space,
        scratch_shapes=[pltpu.SemaphoreType.DMA],
        compiler_params=pltpu.CompilerParams(vmem_limit_bytes=1024 * 1024),
    )(pltpu.with_memory_space_constraint(memory[0], pltpu.HBM), other)
    arrived, keep, other, state = lax.optimization_barrier((arrived, keep, other, state))
    cell, keys, vals, keeps, new_normalizer, new_stabilizer = call(
        cell_kernel,
        [
            ((kv, 16, LANES), BF16),
            ((8, DQK), F32),
            ((8, DV), F32),
            ((8, LANES), F32),
            ((8, DQK), F32),
            ((1, 8), F32),
        ],
        tp_pos,
        arrived,
        state,
        state_norm,
        old_stab,
        ibias,
        fbias,
        scalars=1,
        away=(4, 5),
    )
    cells = lax.all_to_all(cell, "kv", 0, 0, tiled=True)
    half, crossing = call(
        output_kernel,
        [((quarter, 2 * rows), BF16), ((thin, 2 * rows), BF16)],
        tp_pos,
        cells,
        w_out,
        scalars=1,
        scratch=[pltpu.VMEM((rows * 16, LANES), F32)],
    )
    middle, own = call(
        middle_kernel,
        [((kv, quarter, 2 * rows), BF16), ((quarter, 2 * rows), BF16)],
        tp_pos,
        half,
        lax.psum(crossing, "tp"),
        own_tokens,
        scalars=1,
    )
    middles = lax.all_to_all(middle, "kv", 0, 0, tiled=True).reshape(kv * quarter, 2 * rows)
    sums = call(up_kernel, [((136, 128), F32)], tp_pos, middles, keep, other, scalars=1)
    far_sums = lax.ppermute(sums, "tp", [(0, 1), (1, 0)])
    new_memory = call(
        update_kernel,
        [(memory.shape[1:], F32)],
        keys,
        vals,
        keeps,
        state,
        fetched=1,
        away=(0,),
        scratch=[pltpu.VMEM(memory.shape[1:], F32), pltpu.SemaphoreType.DMA((8,))],
    )
    downs = call(
        down_kernel,
        [((kv * quarter, 2 * rows), BF16)],
        tp_pos,
        sums,
        far_sums,
        keep,
        other,
        scalars=1,
    )
    back = lax.all_to_all(downs.reshape(kv, quarter, 2 * rows), "kv", 0, 0, tiled=True)
    new_tokens = call(finish_kernel, [((thin, rows), BF16)], back, own, away=(0,)).T
    return (new_tokens, new_memory[None], new_normalizer[None], new_stabilizer)


def solution(mesh):
    in_specs = (
        P("dp", ("kv", "tp")),
        P(),
        P("kv", "tp"),
        P("kv", "tp"),
        P("kv", "tp"),
        P(),
        P(),
        P(),
        P(),
        P(("dp", "kv"), "tp", None, None),
        P(("dp", "kv"), "tp", None),
        P(("dp", "kv"), "tp"),
        P("tp", "kv"),
        P(),
        P(None, ("kv", "tp")),
        P(("kv", "tp"), None),
    )
    out_specs = (
        P("dp", ("kv", "tp")),
        P(("dp", "kv"), "tp", None, None),
        P(("dp", "kv"), "tp", None),
        P(("dp", "kv"), "tp"),
    )
    return jax.shard_map(on_device, mesh=mesh, in_specs=in_specs, out_specs=out_specs, check_vma=False)
```
